512 devices in a mesh: ep: 128 (over z, x, core), tp: 4 (over y).
Axes of the slice: x: 4, y: 4, z: 16, core: 2. Of those that a mesh axis runs over, the one named last changes fastest.
Arguments:
- tokens: bfloat16 [1024, 1024], P('ep'), may hold values from -6 to 6
- kv_cache: bfloat16 [1024, 4, 1024, 128], P('ep', 'tp'), may hold values from -6 to 6
- lengths: int32 [1024], P('ep'), may hold values from 256 to 1024
- w_query: bfloat16 [1024, 512], P(None, 'tp'), may hold values from -0.1875 to 0.1875
- w_key: bfloat16 [1024, 256], P(None, 'tp'), may hold values from -0.1875 to 0.1875
- w_value: bfloat16 [1024, 256], P(None, 'tp'), may hold values from -0.1875 to 0.1875
- break_bias: float32 [8], P('tp'), may hold values from -7.5 to -3.5
- head_gain: float32 [512], P('tp'), may hold values from 0.1 to 1.9
- w_output: bfloat16 [512, 1024], P('tp'), may hold values from -0.25 to 0.25
- attn_norm_gain: float32 [1024], replicated, may hold values from 0.1 to 1.9
- w_router: bfloat16 [1024, 16], replicated, may hold values from -0.1875 to 0.1875
- routes: int32 [1024, 2], P('ep'), may hold values from 0 to 15, all different within a row; in each aligned block of 8 rows (0 to 7, 8 to 15, ...) at most 2 rows name the same one
- expert_gate: bfloat16 [1024, 57344], P(None, ('ep', 'tp')), may hold values from -0.1875 to 0.1875
- expert_up: bfloat16 [1024, 57344], P(None, ('ep', 'tp')), may hold values from -0.1875 to 0.1875
- expert_down: bfloat16 [57344, 1024], P(('ep', 'tp')), may hold values from -0.09375 to 0.09375
- dense_gate: bfloat16 [1024, 2816], P(None, 'ep'), may hold values from -0.1875 to 0.1875
- dense_up: bfloat16 [1024, 2816], P(None, 'ep'), may hold values from -0.1875 to 0.1875
- dense_down: bfloat16 [2816, 1024], P('ep', 'tp'), may hold values from -0.109375 to 0.109375
- mix_gate: bfloat16 [1024], replicated, may hold values from -0.1875 to 0.1875
- ffn_norm_gain: float32 [1024], P('tp'), may hold values from 0.1 to 1.9
Outputs:
- layer_out: bfloat16 [1024, 1024], P('ep', 'tp')
- new_kv: bfloat16 [1024, 4, 128], P('ep', 'tp')
The draws below stay inside these ranges and needn't reach their ends.
Inputs may be any that keep to these rules, and one draw needn't show every extreme that they name: lengths[b] is the number of valid cached positions of sequence b and the new token's position. `routes`: each row names 2 different experts. Among the rows of one index of ep (aligned blocks of 8 rows) no expert is named more than 2 times, a bound that some block reaches.
All inputs are finite; a program needn't handle non-finite values.
Results may differ from the reference program's by a relative error of at most 0.012.
Values may be sent and summed in bfloat16 or wider, within the bound.
A program may use at most 128 MiB of HBM per device.

```python
import math
import jax
import jax.numpy as jnp
import numpy as np
from jax import lax

D = 1024
H = 8
KV = 4
HD = 64
L = 1024
SEQ_DEV = 8
EXPERTS = 16
TOPK = 2
FE = 3584
FFD = 2816
CAP = 2
SEQS = 1024


def touch_ends(array, rng, low, largest):
    shape = array.shape
    spot = [jax.random.randint(jax.random.fold_in(rng, axis), (), 0, shape[axis]) for axis in range(len(shape))]
    array = array.at[tuple(spot)].set(low)
    longest = shape.index(max(shape))
    spot[longest] = (spot[longest] + 1) % shape[longest]
    return array.at[tuple(spot)].set(largest)


def shard_levels(stream_key, dims, cuts, smallest, top_value):
    level = 1.0
    for dim, shards_of in cuts:
        draws = jax.random.uniform(jax.random.fold_in(jax.random.fold_in(stream_key, 6), dim), (shards_of,), jnp.float32, smallest / len(cuts), top_value / len(cuts))
        level = level * jnp.repeat(jnp.exp(draws), dims[dim] // shards_of).reshape((-1,) + (1,) * (len(dims) - 1 - dim))
    return level


def assign_block(rng, own, number, rows, amount, top, reach, skew):
    ranking = jax.random.permutation(rng, amount)
    crowded, ordinary = load_shares(amount, rows * top, reach, skew, True), load_shares(amount, rows * top, reach, skew, False)
    places = jnp.arange(amount)

    def named(sizes, rotation):
        used = int((sizes > 0).sum())
        fixed = max(1, used // 4)
        moved = fixed + (places - fixed + rotation * (used - fixed)) % max(1, amount - fixed)
        return jnp.zeros((amount,), jnp.int32).at[ranking[jnp.where(places < fixed, places, moved)]].set(jnp.asarray(sizes, jnp.int32))

    sizes = jnp.where(number % 4 == 0, named(crowded, number // 4), named(ordinary, number - number // 4 - 1))
    mixed = jax.random.permutation(jax.random.fold_in(own, 3), amount)
    donor, sink = mixed[0:amount // 2 * 2:2], mixed[1:amount // 2 * 2:2]
    slack = jnp.minimum(sizes[donor] - 1, reach - sizes[sink]) // 2
    slack = jnp.where((donor == ranking[0]) | (sink == ranking[0]) | (sizes[sink] == 0), 0, jnp.maximum(slack, 0))
    moved = jax.random.randint(jax.random.fold_in(own, 4), (amount // 2,), 0, 1 << 20) % (slack + 1)
    sizes = sizes.at[donor].add(-moved).at[sink].add(moved)
    members = jnp.searchsorted(jnp.cumsum(sizes), jnp.arange(rows * top), side="right").astype(jnp.int32)
    listing = members.reshape(top, rows).T
    listing = listing[jax.random.permutation(jax.random.fold_in(own, 1), rows)]
    rotation = jax.random.randint(jax.random.fold_in(own, 2), (rows, 1), 0, top)
    return jnp.take_along_axis(listing, (jnp.arange(top)[None, :] + rotation) % top, axis=1)


def load_shares(count, total, limit, lean, full):
    loads = [(1 << 20) // math.isqrt(rank ** lean) + 1 for rank in range(1, count + 1)]
    largest = limit if full else min(limit, max(-(-total // count), total * loads[0] // sum(loads)))
    least = 1 if total - largest >= count - 1 else 0
    counts, surplus = [largest] + [least] * (count - 1), total - largest - least * (count - 1)
    while surplus > 0:
        free = [i for i in range(1, count) if counts[i] < largest] or [i for i in range(1, count) if counts[i] < limit]
        whole, left = sum([loads[i] for i in free]), surplus
        for i in free:
            addition = min(limit - counts[i], max(1, left * loads[i] // whole), surplus)
            counts[i] = counts[i] + addition
            surplus = surplus - addition
    return np.array(counts)


def normal_values(key, extent, scale, reach, pieces=(), kind=jnp.bfloat16):
    array = jax.random.normal(key, extent, jnp.float32) * scale
    if len(pieces) > 0:
        array = shard_levels(key, extent, pieces, -0.22, 0.18) * array
    return jnp.clip(array, min=-reach, max=reach).astype(kind)


def setup_inputs(seed: int = 0) -> dict:
    key_list = jax.random.split(jax.random.key(seed), 21)
    tokens = normal_values(key_list[0], (SEQS, D), 1.0, 6.0, ((0, 128),))
    kv_cache = normal_values(key_list[1], (SEQS, KV, L, 2 * HD), 1.0, 6.0, ((0, 128), (1, 4)))
    lengths = touch_ends(jax.random.randint(key_list[2], (SEQS,), L // 4, L + 1), jax.random.fold_in(key_list[2], 1), L // 4, L).astype(jnp.int32)
    w_query = normal_values(key_list[3], (D, H * HD), D ** -0.5, 0.1875, ((1, 4),))
    w_key = normal_values(key_list[4], (D, KV * HD), D ** -0.5, 0.1875, ((1, 4),))
    w_value = normal_values(key_list[5], (D, KV * HD), D ** -0.5, 0.1875, ((1, 4),))
    break_bias = jnp.clip(-7.5 + 4.0 * jax.random.uniform(key_list[6], (H,), jnp.float32) ** shard_levels(key_list[6], (H,), ((0, 4),), -0.2, 0.2), -7.5, -3.5)
    head_gain = jnp.clip(1.0 + 0.18 * jax.random.normal(key_list[7], (H * HD,), jnp.float32), 0.1, 1.9)
    w_output = normal_values(key_list[8], (H * HD, D), (H * HD) ** -0.5, 0.25, ((0, 4),))
    attn_norm_gain = jnp.clip(1.0 + 0.18 * jax.random.normal(key_list[9], (D,), jnp.float32), 0.1, 1.9)
    w_router = normal_values(key_list[10], (D, EXPERTS), D ** -0.5, 0.1875)
    routes_keys = jax.random.split(jax.random.fold_in(key_list[11], 1), SEQS // SEQ_DEV)
    routes_turns = jax.random.permutation(jax.random.fold_in(key_list[11], 3), SEQS // SEQ_DEV)
    routes = jax.vmap(lambda own, number: assign_block(jax.random.fold_in(key_list[11], 2), own, number, SEQ_DEV, EXPERTS, TOPK, CAP, 2))(routes_keys, routes_turns).reshape((SEQS, TOPK))
    expert_gate = normal_values(key_list[12], (D, EXPERTS * FE), D ** -0.5, 0.1875, ((1, 512),))
    expert_up = normal_values(key_list[13], (D, EXPERTS * FE), D ** -0.5, 0.1875, ((1, 512),))
    expert_down = normal_values(key_list[14], (EXPERTS * FE, D), FE ** -0.5, 0.09375, ((0, 512),))
    dense_gate = normal_values(key_list[15], (D, FFD), D ** -0.5, 0.1875, ((1, 128),))
    dense_up = normal_values(key_list[16], (D, FFD), D ** -0.5, 0.1875, ((1, 128),))
    dense_down = normal_values(key_list[17], (FFD, D), FFD ** -0.5, 0.109375, ((0, 128), (1, 4)))
    mix_gate = normal_values(key_list[18], (D,), D ** -0.5, 0.1875)
    ffn_norm_gain = jnp.clip(1.0 + 0.18 * jax.random.normal(key_list[19], (D,), jnp.float32), 0.1, 1.9)
    return dict(tokens=tokens, kv_cache=kv_cache, lengths=lengths, w_query=w_query, w_key=w_key, w_value=w_value, break_bias=break_bias, head_gain=head_gain, w_output=w_output, attn_norm_gain=attn_norm_gain, w_router=w_router, routes=routes, expert_gate=expert_gate, expert_up=expert_up, expert_down=expert_down, dense_gate=dense_gate, dense_up=dense_up, dense_down=dense_down, mix_gate=mix_gate, ffn_norm_gain=ffn_norm_gain)


RESIDUAL_SCALE = 8.0 ** 0.25

def layer_norm(values, gain):
    centre = lax.optimization_barrier(jnp.mean(values, axis=-1, keepdims=True))
    centred = values - centre
    spread = lax.optimization_barrier(jnp.mean(centred * centred, axis=-1, keepdims=True))
    return centred * lax.rsqrt(spread + 1e-05) * gain

def reference(tokens, kv_cache, lengths, w_query, w_key, w_value, break_bias, head_gain, w_output, attn_norm_gain, w_router, routes, expert_gate, expert_up, expert_down, dense_gate, dense_up, dense_down, mix_gate, ffn_norm_gain):
    seq_count = tokens.shape[0]
    group_size = H // KV
    blocks = seq_count // SEQ_DEV
    queries = jnp.dot(tokens, w_query, preferred_element_type=jnp.float32).astype(jnp.bfloat16)
    key_new = jnp.dot(tokens, w_key, preferred_element_type=jnp.float32).astype(jnp.bfloat16).reshape(seq_count, KV, HD)
    value_new = jnp.dot(tokens, w_value, preferred_element_type=jnp.float32).astype(jnp.bfloat16).reshape(seq_count, KV, HD)
    new_kv = jnp.concatenate([key_new, value_new], axis=2)
    bias_grid = break_bias.reshape(1, KV, group_size, 1)

    def attend(block_args):
        query_block, cache_block, length = block_args
        query_wide = query_block.reshape(-1, KV, group_size, HD).astype(jnp.float32)
        cached_keys = cache_block[..., :HD].astype(jnp.float32)
        value_rows = cache_block[..., HD:].astype(jnp.float32)
        scores = jnp.einsum('bgqd,bgld->bgql', query_wide, cached_keys) * HD ** (-0.5) + bias_grid
        visible = jnp.arange(L, dtype=jnp.int32)[None, None, None, :] < length[:, None, None, None]
        survive = jnp.where(visible, jax.nn.log_sigmoid(-scores), 0.0)
        remaining = lax.cumsum(survive, axis=3, reverse=True) - survive
        weights = jnp.where(visible, jnp.exp(jax.nn.log_sigmoid(scores) + remaining), 0.0).astype(jnp.bfloat16)
        blended = jnp.einsum('bgql,bgld->bgqd', weights.astype(jnp.float32), value_rows)
        rescale = lax.rsqrt(lax.optimization_barrier(jnp.mean(blended * blended, axis=3, keepdims=True)) + 1e-06)
        return ((blended * rescale).reshape(-1, H * HD) * head_gain).astype(jnp.bfloat16)
    normed = lax.map(attend, (queries.reshape(blocks, SEQ_DEV, H * HD), kv_cache.reshape(blocks, SEQ_DEV, KV, L, 2 * HD), lengths.reshape(blocks, SEQ_DEV)))
    normed = normed.reshape(seq_count, H * HD)
    attended = jnp.dot(normed, w_output, preferred_element_type=jnp.float32)
    settled = layer_norm(RESIDUAL_SCALE * tokens.astype(jnp.float32) + attended, attn_norm_gain).astype(jnp.bfloat16)
    logits = jnp.dot(settled, w_router, preferred_element_type=jnp.float32)
    picked = jnp.take_along_axis(logits, routes, axis=1)
    route_weight = jax.nn.sigmoid(picked - picked[:, ::-1])
    block_routes = routes.reshape(blocks, SEQ_DEV * TOPK)
    assigned = (block_routes[:, :, None] == jnp.arange(EXPERTS, dtype=jnp.int32)[None, None, :]).astype(jnp.int32)
    before = (jnp.cumsum(assigned, axis=1) - assigned).astype(jnp.int32)
    slot_index = lax.optimization_barrier(jnp.sum(before * assigned, axis=2)).astype(jnp.int32)
    position = (jnp.arange(blocks, dtype=jnp.int32)[:, None] * CAP + slot_index).reshape(-1).astype(jnp.int32)
    expert_flat = routes.reshape(-1).astype(jnp.int32)
    token_flat = jnp.repeat(jnp.arange(seq_count, dtype=jnp.int32), TOPK)
    slot_table = jnp.zeros((EXPERTS, blocks * CAP), jnp.int32).at[expert_flat, position].set(token_flat)
    gate_stack = expert_gate.reshape(D, EXPERTS, FE).transpose(1, 0, 2)
    up_stack = expert_up.reshape(D, EXPERTS, FE).transpose(1, 0, 2)
    down_stack = expert_down.reshape(EXPERTS, FE, D)

    def serve_rows(block_args):
        row_index, gate_weight, up_weight, down_weight = block_args
        received = settled[row_index]
        gate_pre = jnp.dot(received, gate_weight, preferred_element_type=jnp.float32)
        up_pre = jnp.dot(received, up_weight, preferred_element_type=jnp.float32)
        hidden = (jax.nn.silu(gate_pre) * up_pre).astype(jnp.bfloat16)
        return jnp.dot(hidden, down_weight, preferred_element_type=jnp.float32)
    served = lax.map(serve_rows, (slot_table, gate_stack, up_stack, down_stack))
    picked_rows = served[expert_flat, position].reshape(seq_count, TOPK, D)
    routed = lax.optimization_barrier(jnp.sum(picked_rows * route_weight[:, :, None], axis=1))
    dense_gate_pre = jnp.dot(settled, dense_gate, preferred_element_type=jnp.float32)
    dense_up_pre = jnp.dot(settled, dense_up, preferred_element_type=jnp.float32)
    dense_hidden = (jax.nn.silu(dense_gate_pre) * dense_up_pre).astype(jnp.bfloat16)
    dense_out = jnp.dot(dense_hidden, dense_down, preferred_element_type=jnp.float32)
    mix_weight = jax.nn.sigmoid(jnp.dot(settled, mix_gate, preferred_element_type=jnp.float32))
    combined = RESIDUAL_SCALE * settled.astype(jnp.float32) + routed + mix_weight[:, None] * dense_out
    return (layer_norm(combined, ffn_norm_gain).astype(jnp.bfloat16), new_kv)
```

```python
import functools

import jax
import jax.numpy as jnp
from jax import lax
from jax.experimental import pallas as pl
from jax.experimental.pallas import tpu as pltpu
from jax.sharding import Mesh
from jax.sharding import PartitionSpec as P

CAP = 2
EP = ("ep_0", "ep_1", "ep_2")
EP_TP = ("ep_0", "ep_1", "ep_2", "tp")
RESIDUAL_SCALE = 8.0**0.25
MESH = pl.DeviceIdType.MESH
F32 = jnp.float32
BF16 = jnp.bfloat16


def nt(a, b):
    return lax.dot_general(a, b, (((1,), (1,)), ((), ())), preferred_element_type=F32)


def nn(a, b):
    return jnp.dot(a, b, preferred_element_type=F32)


def iota(shape, dim):
    return lax.broadcasted_iota(jnp.int32, shape, dim)


def layer_kernel(
    dims,
    tokens_hbm,
    kv_hbm,
    lengths_ref,
    wq_hbm,
    wk_hbm,
    wv_hbm,
    bias_ref,
    head_gain_ref,
    wo_hbm,
    attn_gain_ref,
    router_hbm,
    routes_ref,
    eg_hbm,
    eu_hbm,
    ed_hbm,
    dg_hbm,
    du_hbm,
    dd_hbm,
    mix_ref,
    ffn_gain_ref,
    out_ref,
    new_kv_ref,
    tok,
    kv,
    wq,
    wkv,
    wo,
    router,
    wg,
    wu,
    wd,
    dg_in,
    du_in,
    dd_in,
    dw,
    att,
    settled_cols,
    rows,
    info,
    xe,
    pb,
    pr,
    fb,
    fr,
    stats,
    load_sem,
    kv_sem,
    weight_sem,
    send_sem,
    recv_sem,
):
    Z, X, C, Y = dims
    z, x, c, y = (lax.axis_index(a) for a in EP_TP)
    T, D = tok.shape
    DY = D // Y
    L = kv.shape[1]
    HD = kv.shape[2] // 2
    XC = X * C
    xc = x * C + c
    other = 1 - c
    sib = (z, x, other, y)

    loads = {}

    def load(name, k, src, dst):
        loads[name] = pltpu.make_async_copy(src, dst, load_sem.at[k])
        loads[name].start()

    load("tok", 0, tokens_hbm, tok)
    load("wq", 1, wq_hbm, wq)
    load("wk", 2, wk_hbm, wkv.at[0])
    load("wv", 3, wv_hbm, wkv.at[1])
    kv_copies = [pltpu.make_async_copy(kv_hbm.at[b], kv.at[b], kv_sem.at[b]) for b in range(T)]
    for copy in kv_copies:
        copy.start()
    load("dg", 4, dg_hbm, dg_in)
    load("du", 5, du_hbm, du_in)
    load("dd", 6, dd_hbm, dd_in)
    load("wo", 7, wo_hbm, wo)
    load("router", 8, router_hbm, router)
    load("eg", 9, eg_hbm, wg.at[c])
    load("eu", 10, eu_hbm, wu.at[c])
    load("ed", 11, ed_hbm, wd.at[c])

    barrier = pltpu.get_barrier_semaphore()

    def tell(device):
        pl.semaphore_signal(barrier, inc=1, device_id=device, device_id_type=MESH)

    def far_first(i):
        half = Z // 2
        step = (i + 1) // 2
        return lax.rem(z + half + step * (1 - 2 * lax.rem(i, 2)) + Z, Z)

    def tell_line(i, _):
        tell((far_first(i), x, c, y))
        return 0

    lax.fori_loop(0, Z - 1, tell_line, 0)
    plane = [(i, j) for i in range(X) for j in range(Y) if (i, j) != (0, 0)]

    def plane_peer(i, j):
        return lax.rem(x + i, X), lax.rem(y + j, Y)

    for i, j in plane:
        px, py = plane_peer(i, j)
        tell((z, px, c, py))
    for i in range(X):
        tell((z, lax.rem(x + i, X), other, y))
    partners = Z - 1 + X * Y - 1 + X

    loads["tok"].wait()
    loads["wq"].wait()
    tokens = tok[...]
    queries = nn(tokens, wq[...]).astype(BF16).astype(F32)
    lane = iota((T, 2 * HD), 1)
    turned = pltpu.roll(queries, HD, 1)
    both = jnp.concatenate(
        [jnp.where(lane < HD, queries, 0.0), jnp.where(lane < HD, turned, 0.0)], axis=0
    ).astype(BF16)
    loads["wk"].wait()
    loads["wv"].wait()
    new_kv_ref[...] = nt(tokens, wkv[...].reshape(2 * HD, D)).astype(BF16)

    R = 2 * T
    row_seq = lax.rem(iota((R, 1), 0), T)
    scores = jnp.zeros((R, L), F32)
    limit = jnp.zeros((R, 1), jnp.int32)
    for b in range(T):
        kv_copies[b].wait()
        scores = jnp.where(row_seq == b, nt(both, kv[b]), scores)
        limit = jnp.where(row_seq == b, lengths_ref[b], limit)
    bias = jnp.where(iota((R, 1), 0) < T, bias_ref[0], bias_ref[1])
    scores = scores * HD ** (-0.5) + bias
    tail = jnp.log1p(jnp.exp(-jnp.abs(scores)))
    visible = iota((R, L), 1) < limit
    survive = jnp.where(visible, jnp.minimum(-scores, 0.0) - tail, 0.0)
    taken = jnp.minimum(scores, 0.0) - tail
    blocks = L // 128
    left = jnp.concatenate([survive[:, k * 128 : (k + 1) * 128] for k in range(blocks)], axis=0)
    later = jnp.where(
        (iota((128, 256), 1) >= 128) | (iota((128, 256), 0) > iota((128, 256), 1)), 1.0, 0.0
    ).astype(BF16)
    sums = jnp.zeros((blocks * R, 256), F32)
    for _ in range(3):
        piece = left.astype(BF16)
        sums = sums + nn(piece, later)
        left = left - piece.astype(F32)
    beyond = jnp.zeros((R, 128), F32)
    parts = []
    for k in reversed(range(blocks)):
        here = slice(k * R, (k + 1) * R)
        span = slice(k * 128, (k + 1) * 128)
        parts.append(
            jnp.where(
                visible[:, span], jnp.exp(taken[:, span] + (sums[here, :128] + beyond)), 0.0
            )
        )
        beyond = beyond + sums[here, 128:]
    weights = jnp.concatenate(parts[::-1], axis=1).astype(BF16)
    blended = jnp.zeros((R, 2 * HD), F32)
    for b in range(T):
        blended = jnp.where(row_seq == b, nn(weights, kv[b]), blended)
    wide = iota((R, 2 * HD), 1)
    square = jnp.sum(jnp.where(wide >= HD, blended * blended, 0.0), axis=1, keepdims=True)
    blended = blended * lax.rsqrt(square / HD + 1e-06)
    heads = jnp.where(lane < HD, pltpu.roll(blended[:T], HD, 1), blended[T:])
    normed = (heads * head_gain_ref[...]).astype(BF16)
    loads["wo"].wait()
    att[y] = nn(normed, wo[...]).astype(BF16)

    pl.semaphore_wait(barrier, partners)

    def send(src, dst, k, device):
        pltpu.make_async_remote_copy(
            src_ref=src,
            dst_ref=dst,
            send_sem=send_sem.at[k],
            recv_sem=recv_sem.at[k],
            device_id=device,
            device_id_type=MESH,
        ).start()

    def arrived(ref, k):
        pltpu.make_async_copy(ref, ref, recv_sem.at[k]).wait()

    def left_here(ref, k):
        pltpu.make_async_copy(ref, ref, send_sem.at[k]).wait()

    for j in range(1, Y):
        send(att.at[y], att.at[y], 0, (z, x, c, lax.rem(y + j, Y)))
    for name in ("eg", "eu", "ed"):
        loads[name].wait()
    send(wg.at[c], wg.at[c], 1, sib)
    send(wu.at[c], wu.at[c], 2, sib)
    send(wd.at[c], wd.at[c], 3, sib)
    for name in ("dg", "du", "dd"):
        loads[name].wait()
    FD = dg_in.shape[0]
    FDP = dw.shape[1]

    def padded(values):
        spare = jnp.zeros((FDP - FD, values.shape[1]), F32)
        return jnp.concatenate([values.astype(F32), spare], axis=0).astype(BF16)

    dw[xc, :, :D] = padded(dg_in[...])
    dw[xc, :, D : 2 * D] = padded(du_in[...])
    dw[xc, :, 2 * D :] = padded(dd_in[...])
    for i in range(X):
        for j in range(C):
            if (i, j) != (0, 0):
                send(dw.at[xc], dw.at[xc], 4, (z, lax.rem(x + i, X), lax.rem(c + j, C), y))

    arrived(att.at[pl.ds(0, Y - 1)], 0)
    attended = att[0].astype(F32)
    for j in range(1, Y):
        attended = attended + att[j].astype(F32)
    gain = jnp.concatenate([attn_gain_ref[k : k + 1, :] for k in range(D // 128)], axis=1)
    values = RESIDUAL_SCALE * tokens.astype(F32) + attended
    centred = values - jnp.mean(values, axis=1, keepdims=True)
    spread = jnp.mean(centred * centred, axis=1, keepdims=True)
    settled = (centred * lax.rsqrt(spread + 1e-05) * gain).astype(BF16)
    for j in range(Y):
        settled_cols[j] = settled[:, j * DY : (j + 1) * DY]
    rows[y, z] = settled_cols[y]

    def send_rows(i, _):
        send(rows.at[y, z], rows.at[y, z], 5, (far_first(i), x, c, y))
        return 0

    lax.fori_loop(0, Z - 1, send_rows, 0)

    loads["router"].wait()
    logits = nt(settled, router[...])
    experts = logits.shape[1]
    mix_row = jnp.concatenate(
        [mix_ref[k : k + 1, :].astype(F32) for k in range(D // 128)], axis=1
    )
    mix = 1.0 / (
        1.0 + jnp.exp(-jnp.sum(settled.astype(F32) * mix_row, axis=1, keepdims=True))
    )
    token_row = iota((T, 1), 0)
    routes = []
    for j in range(2):
        column = jnp.zeros((T, 1), jnp.int32)
        for t in range(T):
            column = jnp.where(token_row == t, routes_ref[j, t], column)
        routes.append(column)
    small = iota((T, experts), 1)
    picked = [
        jnp.sum(jnp.where(small == r, logits, 0.0), axis=1, keepdims=True) for r in routes
    ]
    share = [1.0 / (1.0 + jnp.exp(picked[1 - j] - picked[j])) for j in range(2)]
    lanes = iota((T, 128), 1)
    lane_expert = lax.rem(lanes, experts)
    lane_group = lanes // experts
    hits = [lane_expert == r for r in routes]
    named = jnp.where(hits[0] | hits[1], 1.0, 0.0)
    before = jnp.zeros((T, 128), F32)
    for t in range(T - 1):
        before = before + jnp.where(token_row > t, named[t : t + 1, :], 0.0)
    lane_slot = lax.rem(lane_group, 2).astype(F32)
    placed = jnp.where(before == lane_slot, named, 0.0)
    placed_share = placed * jnp.where(hits[0], share[0], share[1])

    def high(v):
        return v.astype(BF16).astype(F32)

    share_high = high(placed_share)
    mix_high = high(mix)
    table = jnp.where(
        lane_group < 2, placed, jnp.where(lane_group < 4, share_high, placed_share - share_high)
    )
    table = jnp.where(
        lanes < 6 * experts,
        table,
        jnp.where(
            lanes == 6 * experts,
            mix_high,
            jnp.where(lanes == 6 * experts + 1, mix - mix_high, 0.0),
        ),
    )
    info[z] = table.astype(BF16)

    def send_info(i, _):
        send(info.at[z], info.at[z], 6, (far_first(i), x, c, y))
        return 0

    lax.fori_loop(0, Z - 1, send_info, 0)

    ZT = Z * T
    ZS = Z * CAP
    arrived(info.at[pl.ds(0, Z - 1)], 6)
    facts = info[...].astype(F32).reshape(ZT, 128).astype(BF16)
    sel_row = iota((ZS, 128), 0)
    sel_pick = jnp.where(iota((ZS, 128), 1) == lax.rem(sel_row, CAP) * experts + z, 1.0, 0.0)
    select = nt(sel_pick.astype(BF16), facts)
    select = jnp.where(
        iota((ZS, ZT), 0) // CAP == iota((ZS, ZT), 1) // T, select, 0.0
    ).astype(BF16)
    share_row = iota((3 * ZS, 128), 0)
    share_group = jnp.where(share_row < 2 * ZS, 2, 4) + lax.rem(share_row, CAP)
    share_pick = jnp.where(iota((3 * ZS, 128), 1) == share_group * experts + z, 1.0, 0.0)
    shares = nt(facts, share_pick.astype(BF16))
    shares = jnp.where(
        iota((ZT, 3 * ZS), 0) // T == lax.rem(iota((ZT, 3 * ZS), 1), ZS) // CAP, shares, 0.0
    ).astype(BF16)
    fact_lane = iota((ZT, 128), 1)
    mixes = jnp.sum(
        jnp.where(
            (fact_lane == 6 * experts) | (fact_lane == 6 * experts + 1), facts.astype(F32), 0.0
        ),
        axis=1,
        keepdims=True,
    )
    arrived(rows.at[y, pl.ds(0, Z - 1)], 5)
    own_rows = rows[y].astype(F32).reshape(ZT, DY).astype(BF16)
    seat = y * X + x
    xe[seat] = nn(select, own_rows).astype(BF16)
    for i, j in plane:
        px, py = plane_peer(i, j)
        send(xe.at[seat], xe.at[seat], 7, (z, px, c, py))
    for j in range(1, Y):
        send(rows.at[y], rows.at[y], 8, (z, x, c, lax.rem(y + j, Y)))

    arrived(wg.at[0], 1)
    arrived(wu.at[0], 2)
    arrived(wd.at[0], 3)
    F = 2 * wg.shape[1]
    gate_t = wg[...].reshape(F, D)
    up_t = wu[...].reshape(F, D)
    down = wd[...].reshape(F, D)
    arrived(xe.at[pl.ds(0, X * Y - 1)], 7)
    received = jnp.concatenate(
        [xe[j * X : (j + 1) * X].reshape(X * ZS, DY) for j in range(Y)], axis=1
    )
    gate_pre = nt(received, gate_t)
    up_pre = nt(received, up_t)
    hidden = (gate_pre / (1.0 + jnp.exp(-gate_pre)) * up_pre).astype(BF16)
    partial = nn(hidden, down).astype(BF16)
    for i in range(X):
        for j in range(Y):
            pb[j * X + i] = partial[i * ZS : (i + 1) * ZS, j * DY : (j + 1) * DY]
    for i, j in plane:
        px, py = plane_peer(i, j)
        send(pb.at[py * X + px], pr.at[seat], 9, (z, px, c, py))
    pr[seat] = pb[seat]

    arrived(dw.at[pl.ds(0, XC - 1)], 4)
    arrived(rows.at[pl.ds(0, Y - 1)], 8)
    FP = XC * FDP
    line = jnp.concatenate(
        [rows[j].astype(F32).reshape(ZT, DY).astype(BF16) for j in range(Y)], axis=1
    )

    def stacked(a, b):
        return jnp.concatenate([dw[k, :, a:b] for k in range(XC)], axis=0)

    dense_gate = nt(line, stacked(0, D))
    dense_up = nt(line, stacked(D, 2 * D))
    dense_hidden = (dense_gate / (1.0 + jnp.exp(-dense_gate)) * dense_up).astype(BF16)
    dense = nn(dense_hidden, stacked(2 * D, 2 * D + DY)) * mixes

    arrived(pr.at[pl.ds(0, X * Y - 1)], 9)
    served = jnp.zeros((ZS, DY), F32)
    for k in range(X * Y):
        served = served + pr[k].astype(F32)
    served_high = served.astype(BF16)
    served_low = (served - served_high.astype(F32)).astype(BF16)
    stack = jnp.concatenate([served_high, served_low, served_high], axis=0)
    mixed = dense + nn(shares, stack)
    fb[...] = mixed.reshape(Z, T, DY).astype(BF16)
    fr[z] = fb[z]

    def send_back(i, _):
        to = far_first(i)
        send(fb.at[to], fr.at[z], 10, (to, x, c, y))
        return 0

    lax.fori_loop(0, Z - 1, send_back, 0)

    arrived(fr.at[pl.ds(0, Z - 1)], 10)
    combined = RESIDUAL_SCALE * settled_cols[y].astype(F32)
    combined = combined + jnp.sum(fr[...].astype(F32), axis=0)
    centre = jnp.sum(combined, axis=1, keepdims=True) / DY
    centred = combined - centre
    scatter = jnp.sum(centred * centred, axis=1, keepdims=True)
    stats[y] = jnp.where(lanes == 0, centre, jnp.where(lanes == 1, scatter, 0.0))
    for j in range(1, Y):
        send(stats.at[y], stats.at[y], 11, (z, x, c, lax.rem(y + j, Y)))
    ffn_gain = jnp.concatenate(
        [ffn_gain_ref[k : k + 1, :] for k in range(DY // 128)], axis=1
    )
    arrived(stats.at[pl.ds(0, Y - 1)], 11)
    every = [stats[j] for j in range(Y)]
    mean = sum(e[:, 0:1] for e in every) / Y
    var = sum(e[:, 1:2] + DY * (e[:, 0:1] - mean) * (e[:, 0:1] - mean) for e in every) / D
    out_ref[...] = ((combined - mean) * lax.rsqrt(var + 1e-05) * ffn_gain).astype(BF16)

    left_here(att.at[pl.ds(0, Y - 1)], 0)
    left_here(wg.at[0], 1)
    left_here(wu.at[0], 2)
    left_here(wd.at[0], 3)
    left_here(dw.at[pl.ds(0, XC - 1)], 4)
    left_here(rows.at[y, pl.ds(0, Z - 1)], 5)
    left_here(info.at[pl.ds(0, Z - 1)], 6)
    left_here(xe.at[pl.ds(0, X * Y - 1)], 7)
    left_here(rows.at[pl.ds(0, Y - 1)], 8)
    left_here(pb.at[pl.ds(0, X * Y - 1)], 9)
    left_here(fb.at[pl.ds(0, Z - 1)], 10)
    left_here(stats.at[pl.ds(0, Y - 1)], 11)


def body(
    dims,
    tokens,
    kv_cache,
    lengths,
    w_query,
    w_key,
    w_value,
    break_bias,
    head_gain,
    w_output,
    attn_norm_gain,
    w_router,
    routes,
    expert_gate,
    expert_up,
    expert_down,
    dense_gate,
    dense_up,
    dense_down,
    mix_gate,
    ffn_norm_gain,
):
    Z, X, C, Y = dims
    T, D = tokens.shape
    DY = D // Y
    L, HD2 = kv_cache.shape[2:]
    F = expert_gate.shape[1]
    FD = dense_gate.shape[1]
    FDP = -(-FD // 8) * 8
    ZS = Z * CAP
    experts = w_router.shape[1]
    anywhere = pl.BlockSpec(memory_space=pl.ANY)
    vmem = pl.BlockSpec(memory_space=pltpu.VMEM)
    smem = pl.BlockSpec(memory_space=pltpu.SMEM)
    V = pltpu.VMEM
    result, new_kv = pl.pallas_call(
        functools.partial(layer_kernel, dims),
        out_shape=(
            jax.ShapeDtypeStruct((T, DY), BF16),
            jax.ShapeDtypeStruct((T, HD2), BF16),
        ),
        in_specs=[
            anywhere,
            anywhere,
            smem,
            anywhere,
            anywhere,
            anywhere,
            smem,
            vmem,
            anywhere,
            vmem,
            anywhere,
            smem,
            anywhere,
            anywhere,
            anywhere,
            anywhere,
            anywhere,
            anywhere,
            vmem,
            vmem,
        ],
        out_specs=(vmem, vmem),
        scratch_shapes=[
            V((T, D), BF16),
            V((T, L, HD2), BF16),
            V((D, HD2), BF16),
            V((2, HD2 // 2, D), BF16),
            V((HD2, D), BF16),
            V((experts, D), BF16),
            V((C, F, D), BF16),
            V((C, F, D), BF16),
            V((C, F, D), BF16),
            V((FD, D), BF16),
            V((FD, D), BF16),
            V((FD, DY), BF16),
            V((X * C, FDP, 2 * D + DY), BF16),
            V((Y, T, D), BF16),
            V((Y, T, DY), BF16),
            V((Y, Z, T, DY), BF16),
            V((Z, T, 128), BF16),
            V((X * Y, ZS, DY), BF16),
            V((X * Y, ZS, DY), BF16),
            V((X * Y, ZS, DY), BF16),
            V((Z, T, DY), BF16),
            V((Z, T, DY), BF16),
            V((Y, T, 128), F32),
            pltpu.SemaphoreType.DMA((12,)),
            pltpu.SemaphoreType.DMA((T,)),
            pltpu.SemaphoreType.DMA((2,)),
            pltpu.SemaphoreType.DMA((12,)),
            pltpu.SemaphoreType.DMA((12,)),
        ],
        compiler_params=pltpu.CompilerParams(
            collective_id=0, has_side_effects=True, vmem_limit_bytes=67043328
        ),
        name="layer",
    )(
        tokens,
        kv_cache.reshape(T, L, HD2),
        lengths,
        w_query,
        w_key.T,
        w_value.T,
        break_bias,
        head_gain.reshape(1, HD2),
        w_output,
        attn_norm_gain.reshape(D // 128, 128),
        w_router.T,
        routes.T,
        expert_gate.T,
        expert_up.T,
        expert_down,
        dense_gate.T,
        dense_up.T,
        dense_down,
        mix_gate.reshape(D // 128, 128),
        ffn_norm_gain.reshape(DY // 128, 128),
    )
    return result, new_kv.reshape(T, 1, HD2)


def solution(mesh):
    cores = 2
    ep, tp = mesh.shape["ep"], mesh.shape["tp"]
    dims = (ep // (4 * cores), 4, cores, tp)
    split = Mesh(mesh.devices.reshape(dims), EP_TP)
    return jax.shard_map(
        functools.partial(body, dims),
        mesh=split,
        in_specs=(
            P(EP, None),
            P(EP, "tp", None, None),
            P(EP),
            P(None, "tp"),
            P(None, "tp"),
            P(None, "tp"),
            P("tp"),
            P("tp"),
            P("tp", None),
            P(),
            P(),
            P(EP, None),
            P(None, EP_TP),
            P(None, EP_TP),
            P(EP_TP, None),
            P(None, EP),
            P(None, EP),
            P(EP, "tp"),
            P(),
            P("tp"),
        ),
        out_specs=(P(EP, "tp"), P(EP, "tp", None)),
        check_vma=False,
    )
```

```python
import functools

import jax
import jax.numpy as jnp
from jax import lax
from jax.experimental import pallas as pl
from jax.experimental.pallas import tpu as pltpu
from jax.sharding import Mesh
from jax.sharding import PartitionSpec as P

CAP = 2
CHUNKS = 2
EP = ("ep_0", "ep_1", "ep_2")
EP_TP = ("ep_0", "ep_1", "ep_2", "tp")
RESIDUAL_SCALE = 8.0**0.25
MESH = pl.DeviceIdType.MESH
F32 = jnp.float32
BF16 = jnp.bfloat16


def nt(a, b):
    return lax.dot_general(a, b, (((1,), (1,)), ((), ())), preferred_element_type=F32)


def nn(a, b):
    return jnp.dot(a, b, preferred_element_type=F32)


def iota(shape, dim):
    return lax.broadcasted_iota(jnp.int32, shape, dim)


def layer_kernel(
    dims,
    tokens_hbm,
    kv_hbm,
    lengths_hbm,
    wq_hbm,
    wk_hbm,
    wv_hbm,
    bias_hbm,
    head_gain_hbm,
    wo_hbm,
    attn_gain_hbm,
    router_hbm,
    routes_hbm,
    eg_hbm,
    eu_hbm,
    ed_hbm,
    dg_hbm,
    du_hbm,
    dd_hbm,
    mix_hbm,
    ffn_gain_hbm,
    out_hbm,
    new_kv_hbm,
    tok,
    kv,
    wq,
    wkv,
    wo,
    router,
    wg,
    wu,
    wd,
    dg_in,
    du_in,
    dd_in,
    dw,
    att,
    settled_cols,
    rows,
    xe,
    pb,
    pr,
    fb,
    fr,
    stats,
    lengths_ref,
    bias_ref,
    routes_ref,
    head_gain_ref,
    attn_gain_ref,
    mix_ref,
    ffn_gain_ref,
    out_ref,
    new_kv_ref,
    load_sem,
    kv_sem,
    send_sem,
    recv_sem,
    hello_line,
    hello_core,
    hello_column,
):
    Z, X, C, Y = dims
    z, x, c, y = (lax.axis_index(a) for a in EP_TP)
    T, D = tok.shape
    DY = D // Y
    L = kv.shape[1]
    HD = kv.shape[2] // 2
    XC = X * C
    xc = x * C + c
    other = 1 - c
    sib = (z, x, other, y)

    loads = {}

    def load(name, k, src, dst):
        loads[name] = pltpu.make_async_copy(src, dst, load_sem.at[k])
        loads[name].start()

    load("tok", 0, tokens_hbm, tok)
    load("wq", 1, wq_hbm, wq)
    load("lengths", 12, lengths_hbm, lengths_ref)
    load("bias", 13, bias_hbm, bias_ref)
    load("wk", 2, wk_hbm, wkv.at[0])
    load("wv", 3, wv_hbm, wkv.at[1])
    kv_copies = [pltpu.make_async_copy(kv_hbm.at[b], kv.at[b], kv_sem.at[b]) for b in range(T)]
    for copy in kv_copies:
        copy.start()
    load("dg", 4, dg_hbm, dg_in)
    load("du", 5, du_hbm, du_in)
    load("dd", 6, dd_hbm, dd_in)
    load("wo", 7, wo_hbm, wo)
    load("router", 8, router_hbm, router)
    load("head_gain", 14, head_gain_hbm, head_gain_ref)
    load("attn_gain", 15, attn_gain_hbm, attn_gain_ref)
    load("routes", 16, routes_hbm, routes_ref)
    load("mix", 17, mix_hbm, mix_ref)
    load("ffn_gain", 18, ffn_gain_hbm, ffn_gain_ref)
    load("eg", 9, eg_hbm, wg.at[c])
    load("eu", 10, eu_hbm, wu.at[c])
    load("ed", 11, ed_hbm, wd.at[c])

    barrier = pltpu.get_barrier_semaphore()

    def tell(sem, device):
        pl.semaphore_signal(sem, inc=1, device_id=device, device_id_type=MESH)

    for j in range(1, Y):
        tell(barrier, (z, x, c, lax.rem(y + j, Y)))
    for i in range(1, X):
        tell(barrier, (z, lax.rem(x + i, X), c, y))

    def tell_later(k, _):
        tell(barrier, (k, x, c, y))
        return 0

    lax.fori_loop(z + 1, Z, tell_later, 0)

    @pl.when(c == 0)
    def _():
        for i in range(X):
            tell(barrier, (z, lax.rem(x + i, X), other, y))

    plane = [(i, j) for i in range(X) for j in range(Y) if (i, j) != (0, 0)]
    plane.sort(key=lambda p: -(min(p[0], X - p[0]) + min(p[1], Y - p[1])))

    def plane_peer(i, j):
        return lax.rem(x + i, X), lax.rem(y + j, Y)

    loads["tok"].wait()
    loads["wq"].wait()
    tokens = tok[...]
    queries = nn(tokens, wq[...]).astype(BF16).astype(F32)
    lane = iota((T, 2 * HD), 1)
    turned = pltpu.roll(queries, HD, 1)
    both = jnp.concatenate(
        [jnp.where(lane < HD, queries, 0.0), jnp.where(lane < HD, turned, 0.0)], axis=0
    ).astype(BF16)
    loads["wk"].wait()
    loads["wv"].wait()
    new_kv_ref[...] = nt(tokens, wkv[...].reshape(2 * HD, D)).astype(BF16)
    put_kv = pltpu.make_async_copy(new_kv_ref, new_kv_hbm, load_sem.at[19])
    put_kv.start()

    loads["lengths"].wait()
    loads["bias"].wait()
    pl.semaphore_wait(barrier, Y - 1 + X - 1 + z + c * X)

    def answer(k, _):
        tell(hello_line.at[z], (k, x, c, y))
        return 0

    lax.fori_loop(0, z, answer, 0)

    @pl.when(c == 1)
    def _():
        for i in range(X):
            tell(hello_core, (z, lax.rem(x + i, X), other, y))

    for i in range(1, X):
        tell(hello_column, (z, lax.rem(x + i, X), c, y))

    R = 2 * T
    row_seq = lax.rem(iota((R, 1), 0), T)
    scores = jnp.zeros((R, L), F32)
    limit = jnp.zeros((R, 1), jnp.int32)
    for b in range(T):
        kv_copies[b].wait()
        scores = jnp.where(row_seq == b, nt(both, kv[b]), scores)
        limit = jnp.where(row_seq == b, lengths_ref[b], limit)
    bias = jnp.where(iota((R, 1), 0) < T, bias_ref[0], bias_ref[1])
    scores = scores * HD ** (-0.5) + bias
    tail = jnp.log1p(jnp.exp(-jnp.abs(scores)))
    visible = iota((R, L), 1) < limit
    survive = jnp.where(visible, jnp.minimum(-scores, 0.0) - tail, 0.0)
    taken = jnp.minimum(scores, 0.0) - tail
    blocks = L // 128
    left = jnp.concatenate([survive[:, k * 128 : (k + 1) * 128] for k in range(blocks)], axis=0)
    later = jnp.where(
        (iota((128, 256), 1) >= 128) | (iota((128, 256), 0) > iota((128, 256), 1)), 1.0, 0.0
    ).astype(BF16)
    sums = jnp.zeros((blocks * R, 256), F32)
    for _ in range(3):
        piece = left.astype(BF16)
        sums = sums + nn(piece, later)
        left = left - piece.astype(F32)
    beyond = jnp.zeros((R, 128), F32)
    parts = []
    for k in reversed(range(blocks)):
        here = slice(k * R, (k + 1) * R)
        span = slice(k * 128, (k + 1) * 128)
        parts.append(
            jnp.where(
                visible[:, span], jnp.exp(taken[:, span] + (sums[here, :128] + beyond)), 0.0
            )
        )
        beyond = beyond + sums[here, 128:]
    weights = jnp.concatenate(parts[::-1], axis=1).astype(BF16)
    blended = jnp.zeros((R, 2 * HD), F32)
    for b in range(T):
        blended = jnp.where(row_seq == b, nn(weights, kv[b]), blended)
    wide = iota((R, 2 * HD), 1)
    square = jnp.sum(jnp.where(wide >= HD, blended * blended, 0.0), axis=1, keepdims=True)
    blended = blended * lax.rsqrt(square / HD + 1e-06)
    heads = jnp.where(lane < HD, pltpu.roll(blended[:T], HD, 1), blended[T:])
    loads["head_gain"].wait()
    normed = (heads * head_gain_ref[...]).astype(BF16)
    loads["wo"].wait()
    att[y] = nn(normed, wo[...]).astype(BF16)


    def send(src, dst, k, device):
        pltpu.make_async_remote_copy(
            src_ref=src,
            dst_ref=dst,
            send_sem=send_sem.at[k],
            recv_sem=recv_sem.at[k],
            device_id=device,
            device_id_type=MESH,
        ).start()

    def arrived(ref, k):
        pltpu.make_async_copy(ref, ref, recv_sem.at[k]).wait()

    def left_here(ref, k):
        pltpu.make_async_copy(ref, ref, send_sem.at[k]).wait()

    for j in range(1, Y):
        send(att.at[y], att.at[y], 0, (z, x, c, lax.rem(y + j, Y)))
    for name in ("dg", "du", "dd"):
        loads[name].wait()
    FD = dg_in.shape[0]
    FDP = dw.shape[1]

    def padded(values):
        spare = jnp.zeros((FDP - FD, values.shape[1]), F32)
        return jnp.concatenate([values.astype(F32), spare], axis=0).astype(BF16)

    dw[xc, :, :D] = padded(dg_in[...])
    dw[xc, :, D : 2 * D] = padded(du_in[...])
    dw[xc, :, 2 * D :] = padded(dd_in[...])
    for i in range(1, X):
        send(dw.at[xc], dw.at[xc], 4, (z, lax.rem(x + i, X), c, y))
    for name in ("eg", "eu", "ed"):
        loads[name].wait()

    @pl.when(c == 0)
    def _():
        pl.semaphore_wait(hello_core, X)

    send(wg.at[c], wg.at[c], 1, sib)
    send(wu.at[c], wu.at[c], 2, sib)
    send(wd.at[c], wd.at[c], 3, sib)
    for i in range(X):
        send(dw.at[xc], dw.at[xc], 4, (z, lax.rem(x + i, X), other, y))

    for name in ("attn_gain", "router", "routes", "mix", "ffn_gain"):
        loads[name].wait()
    token_row = iota((T, 1), 0)
    routes = []
    for j in range(2):
        column = jnp.zeros((T, 1), jnp.int32)
        for t in range(T):
            column = jnp.where(token_row == t, routes_ref[j, t], column)
        routes.append(column)
    experts = router.shape[0]
    lanes = iota((T, 128), 1)
    lane_expert = lax.rem(lanes, experts)
    lane_group = lanes // experts
    hits = [lane_expert == r for r in routes]
    named = jnp.where(hits[0] | hits[1], 1.0, 0.0)
    before = jnp.zeros((T, 128), F32)
    for t in range(T - 1):
        before = before + jnp.where(token_row > t, named[t : t + 1, :], 0.0)
    lane_slot = lax.rem(lane_group, 2).astype(F32)
    placed = jnp.where(before == lane_slot, named, 0.0)
    mix_row = jnp.concatenate(
        [mix_ref[k : k + 1, :].astype(F32) for k in range(D // 128)], axis=1
    )
    arrived(att.at[pl.ds(0, Y - 1)], 0)
    attended = att[0].astype(F32)
    for j in range(1, Y):
        attended = attended + att[j].astype(F32)
    gain = jnp.concatenate([attn_gain_ref[k : k + 1, :] for k in range(D // 128)], axis=1)
    values = RESIDUAL_SCALE * tokens.astype(F32) + attended
    centred = values - jnp.mean(values, axis=1, keepdims=True)
    spread = jnp.mean(centred * centred, axis=1, keepdims=True)
    settled = (centred * lax.rsqrt(spread + 1e-05) * gain).astype(BF16)
    for j in range(Y):
        settled_cols[j] = settled[:, j * DY : (j + 1) * DY]
    logits = nt(settled, router[...])
    mix = 1.0 / (
        1.0 + jnp.exp(-jnp.sum(settled.astype(F32) * mix_row, axis=1, keepdims=True))
    )
    small = iota((T, experts), 1)
    picked = [
        jnp.sum(jnp.where(small == r, logits, 0.0), axis=1, keepdims=True) for r in routes
    ]
    share = [1.0 / (1.0 + jnp.exp(picked[1 - j] - picked[j])) for j in range(2)]
    placed_share = placed * jnp.where(hits[0], share[0], share[1])

    def high(v):
        return v.astype(BF16).astype(F32)

    share_high = high(placed_share)
    mix_high = high(mix)
    table = jnp.where(
        lane_group < 2, placed, jnp.where(lane_group < 4, share_high, placed_share - share_high)
    )
    table = jnp.where(
        lanes < 6 * experts,
        table,
        jnp.where(
            lanes == 6 * experts,
            mix_high,
            jnp.where(lanes == 6 * experts + 1, mix - mix_high, 0.0),
        ),
    )
    rows[y, z, :, DY:] = table.astype(BF16)
    rows[y, z, :, :DY] = settled_cols[y]

    def send_rows(k, _):
        send(rows.at[y, z], rows.at[y, z], 16 + z // (Z // CHUNKS), (k, x, c, y))
        return 0

    def send_rows_later(k, _):
        pl.semaphore_wait(hello_line.at[k], 1)
        return send_rows(k, 0)

    lax.fori_loop(0, z, send_rows, 0)
    lax.fori_loop(z + 1, Z, send_rows_later, 0)
    pl.semaphore_wait(hello_column, X - 1)

    ZC = Z // CHUNKS
    TC = ZC * T
    SC = ZC * CAP
    seat = y * X + x
    sel_row = iota((SC, 128), 0)
    sel_pick = jnp.where(
        iota((SC, 128), 1) == lax.rem(sel_row, CAP) * experts + z, 1.0, 0.0
    ).astype(BF16)
    sel_mask = iota((SC, TC), 0) // CAP == iota((SC, TC), 1) // T
    share_row = iota((3 * SC, 128), 0)
    share_group = jnp.where(share_row < 2 * SC, 2, 4) + lax.rem(share_row, CAP)
    share_pick = jnp.where(
        iota((3 * SC, 128), 1) == share_group * experts + z, 1.0, 0.0
    ).astype(BF16)
    share_mask = iota((TC, 3 * SC), 0) // T == lax.rem(iota((TC, 3 * SC), 1), SC) // CAP
    fact_lane = iota((TC, 128), 1)
    mix_lanes = (fact_lane == 6 * experts) | (fact_lane == 6 * experts + 1)
    F = 2 * wg.shape[1]
    mixing = {}

    def arrived_line(buf, g, k):
        first = g * ZC

        @pl.when(z // ZC == g)
        def _():
            if ZC > 1:
                arrived(buf.at[pl.ds(first, ZC - 1)], k)

        @pl.when(z // ZC != g)
        def _():
            arrived(buf.at[pl.ds(first, ZC)], k)

    def gather(g):
        first = g * ZC
        arrived_line(rows.at[y], g, 16 + g)
        facts = rows[y, first : first + ZC, :, DY:].astype(F32).reshape(TC, 128).astype(BF16)
        select = jnp.where(sel_mask, nt(sel_pick, facts), 0.0).astype(BF16)
        own = rows[y, first : first + ZC, :, :DY].astype(F32).reshape(TC, DY).astype(BF16)
        xe[g, seat] = nn(select, own).astype(BF16)
        for i, j in plane:
            px, py = plane_peer(i, j)
            send(xe.at[g, seat], xe.at[g, seat], 24 + g, (z, px, c, py))
        shares = jnp.where(share_mask, nt(facts, share_pick), 0.0).astype(BF16)
        mixes = jnp.sum(
            jnp.where(mix_lanes, facts.astype(F32), 0.0), axis=1, keepdims=True
        )
        mixing[g] = (shares, mixes)

    def expert(g):
        arrived(xe.at[g, pl.ds(0, X * Y - 1)], 24 + g)
        received = jnp.concatenate(
            [
                xe[g, j * X : (j + 1) * X].astype(F32).reshape(X * SC, DY).astype(BF16)
                for j in range(Y)
            ],
            axis=1,
        )
        gate_pre = nt(received, wg[...].reshape(F, D))
        up_pre = nt(received, wu[...].reshape(F, D))
        hidden = (gate_pre / (1.0 + jnp.exp(-gate_pre)) * up_pre).astype(BF16)
        partial = nn(hidden, wd[...].reshape(F, D))
        for i in range(X):
            for j in range(Y):
                pb[g, j * X + i] = partial[
                    i * SC : (i + 1) * SC, j * DY : (j + 1) * DY
                ].astype(BF16)
        for i, j in plane:
            px, py = plane_peer(i, j)
            send(pb.at[g, py * X + px], pr.at[g, seat], 32 + g, (z, px, c, py))
        pr[g, seat] = pb[g, seat]

    def stacked(a, b):
        return jnp.concatenate([dw[k, :, a:b] for k in range(XC)], axis=0)

    def dense_part(g):
        first = g * ZC
        arrived(rows.at[pl.ds(0, Y - 1), pl.ds(first, ZC), :, pl.ds(0, DY)], 28 + g)
        line = jnp.concatenate(
            [
                rows[j, first : first + ZC, :, :DY].astype(F32).reshape(TC, DY).astype(BF16)
                for j in range(Y)
            ],
            axis=1,
        )
        dense_gate = nt(line, stacked(0, D))
        dense_up = nt(line, stacked(D, 2 * D))
        dense_hidden = (dense_gate / (1.0 + jnp.exp(-dense_gate)) * dense_up).astype(BF16)
        shares, mixes = mixing[g]
        mixing[g] = (shares, nn(dense_hidden, stacked(2 * D, 2 * D + DY)) * mixes)

    def home(g):
        first = g * ZC
        arrived(pr.at[g, pl.ds(0, X * Y - 1)], 32 + g)
        served = jnp.zeros((SC, DY), F32)
        for k in range(X * Y):
            served = served + pr[g, k].astype(F32)
        served_high = served.astype(BF16)
        served_low = (served - served_high.astype(F32)).astype(BF16)
        stack = jnp.concatenate([served_high, served_low, served_high], axis=0)
        shares, dense = mixing[g]
        mixed = dense + nn(shares, stack)
        fb[first : first + ZC] = mixed.reshape(ZC, T, DY).astype(BF16)
        for to in range(first, first + ZC):

            @pl.when(z != to)
            def _(to=to):
                send(fb.at[to], fr.at[z], 10, (to, x, c, y))

            @pl.when(z == to)
            def _(to=to):
                fr[to] = fb[to]

    for g in range(CHUNKS):
        gather(g)
    for g in range(CHUNKS):
        for j in range(1, Y):
            block = rows.at[y, pl.ds(g * ZC, ZC), :, pl.ds(0, DY)]
            send(block, block, 28 + g, (z, x, c, lax.rem(y + j, Y)))
    arrived(wg.at[0], 1)
    arrived(wu.at[0], 2)
    arrived(wd.at[0], 3)
    for g in range(CHUNKS):
        expert(g)
    arrived(dw.at[pl.ds(0, XC - 1)], 4)
    for g in range(CHUNKS):
        dense_part(g)
    for g in range(CHUNKS):
        home(g)

    arrived(fr.at[pl.ds(0, Z - 1)], 10)
    combined = RESIDUAL_SCALE * settled_cols[y].astype(F32)
    combined = combined + jnp.sum(fr[...].astype(F32), axis=0)
    centre = jnp.sum(combined, axis=1, keepdims=True) / DY
    centred = combined - centre
    scatter = jnp.sum(centred * centred, axis=1, keepdims=True)
    stats[y] = jnp.where(lanes == 0, centre, jnp.where(lanes == 1, scatter, 0.0))
    for j in range(1, Y):
        send(stats.at[y], stats.at[y], 11, (z, x, c, lax.rem(y + j, Y)))
    ffn_gain = jnp.concatenate(
        [ffn_gain_ref[k : k + 1, :] for k in range(DY // 128)], axis=1
    )
    arrived(stats.at[pl.ds(0, Y - 1)], 11)
    every = [stats[j] for j in range(Y)]
    mean = sum(e[:, 0:1] for e in every) / Y
    var = sum(e[:, 1:2] + DY * (e[:, 0:1] - mean) * (e[:, 0:1] - mean) for e in every) / D
    out_ref[...] = ((combined - mean) * lax.rsqrt(var + 1e-05) * ffn_gain).astype(BF16)

    put = pltpu.make_async_copy(out_ref, out_hbm, load_sem.at[20])
    put.start()

    left_here(att.at[pl.ds(0, Y - 1)], 0)
    left_here(wg.at[0], 1)
    left_here(wu.at[0], 2)
    left_here(wd.at[0], 3)
    left_here(dw.at[pl.ds(0, XC - 1)], 4)
    left_here(rows.at[y, pl.ds(0, Z - 1)], 16 + z // ZC)
    for g in range(CHUNKS):
        left_here(xe.at[g, pl.ds(0, X * Y - 1)], 24 + g)
        left_here(rows.at[pl.ds(0, Y - 1), pl.ds(g * ZC, ZC), :, pl.ds(0, DY)], 28 + g)
        left_here(pb.at[g, pl.ds(0, X * Y - 1)], 32 + g)
    left_here(fb.at[pl.ds(0, Z - 1)], 10)
    left_here(stats.at[pl.ds(0, Y - 1)], 11)
    put_kv.wait()
    put.wait()


def hand_over(result_in, kv_in, result_out, kv_out, sem):
    copies = [
        pltpu.make_async_copy(result_in, result_out, sem.at[0]),
        pltpu.make_async_copy(kv_in, kv_out, sem.at[1]),
    ]
    for copy in copies:
        copy.start()
    for copy in copies:
        copy.wait()


def body(
    dims,
    tokens,
    kv_cache,
    lengths,
    w_query,
    w_key,
    w_value,
    break_bias,
    head_gain,
    w_output,
    attn_norm_gain,
    w_router,
    routes,
    expert_gate,
    expert_up,
    expert_down,
    dense_gate,
    dense_up,
    dense_down,
    mix_gate,
    ffn_norm_gain,
):
    Z, X, C, Y = dims
    T, D = tokens.shape
    DY = D // Y
    L, HD2 = kv_cache.shape[2:]
    F = expert_gate.shape[1]
    FD = dense_gate.shape[1]
    FDP = -(-FD // 8) * 8
    ZS = Z * CAP
    experts = w_router.shape[1]
    anywhere = pl.BlockSpec(memory_space=pl.ANY)
    V = pltpu.VMEM
    result, new_kv = pl.pallas_call(
        functools.partial(layer_kernel, dims),
        out_shape=(
            jax.ShapeDtypeStruct((T, DY), BF16),
            jax.ShapeDtypeStruct((T, HD2), BF16),
        ),
        in_specs=[anywhere] * 20,
        out_specs=(anywhere, anywhere),
        scratch_shapes=[
            V((T, D), BF16),
            V((T, L, HD2), BF16),
            V((D, HD2), BF16),
            V((2, HD2 // 2, D), BF16),
            V((HD2, D), BF16),
            V((experts, D), BF16),
            V((C, F, D), BF16),
            V((C, F, D), BF16),
            V((C, F, D), BF16),
            V((FD, D), BF16),
            V((FD, D), BF16),
            V((FD, DY), BF16),
            V((X * C, FDP, 2 * D + DY), BF16),
            V((Y, T, D), BF16),
            V((Y, T, DY), BF16),
            V((Y, Z, T, DY + 128), BF16),
            V((CHUNKS, X * Y, ZS // CHUNKS, DY), BF16),
            V((CHUNKS, X * Y, ZS // CHUNKS, DY), BF16),
            V((CHUNKS, X * Y, ZS // CHUNKS, DY), BF16),
            V((Z, T, DY), BF16),
            V((Z, T, DY), BF16),
            V((Y, T, 128), F32),
            pltpu.SMEM((T,), jnp.int32),
            pltpu.SMEM((2,), F32),
            pltpu.SMEM((2, T), jnp.int32),
            V((1, HD2), F32),
            V((D // 128, 128), F32),
            V((D // 128, 128), BF16),
            V((DY // 128, 128), F32),
            V((T, DY), BF16),
            V((T, HD2), BF16),
            pltpu.SemaphoreType.DMA((21,)),
            pltpu.SemaphoreType.DMA((T,)),
            pltpu.SemaphoreType.DMA((36,)),
            pltpu.SemaphoreType.DMA((36,)),
            pltpu.SemaphoreType.REGULAR((dims[0],)),
            pltpu.SemaphoreType.REGULAR,
            pltpu.SemaphoreType.REGULAR,
        ],
        compiler_params=pltpu.CompilerParams(
            collective_id=0, has_side_effects=True, vmem_limit_bytes=67043328
        ),
        name="layer",
    )(
        tokens,
        kv_cache.reshape(T, L, HD2),
        lengths,
        w_query,
        w_key.T,
        w_value.T,
        break_bias,
        head_gain.reshape(1, HD2),
        w_output,
        attn_norm_gain.reshape(D // 128, 128),
        w_router.T,
        routes.T,
        expert_gate.T,
        expert_up.T,
        expert_down,
        dense_gate.T,
        dense_up.T,
        dense_down,
        mix_gate.reshape(D // 128, 128),
        ffn_norm_gain.reshape(DY // 128, 128),
    )
    result, new_kv = pl.pallas_call(
        hand_over,
        out_shape=(
            jax.ShapeDtypeStruct((T, DY), BF16),
            jax.ShapeDtypeStruct((T, HD2), BF16),
        ),
        in_specs=[anywhere] * 2,
        out_specs=(anywhere, anywhere),
        scratch_shapes=[pltpu.SemaphoreType.DMA((2,))],
        name="hand_over",
    )(result, new_kv)
    return result, new_kv.reshape(T, 1, HD2)


def solution(mesh):
    cores = 2
    ep, tp = mesh.shape["ep"], mesh.shape["tp"]
    dims = (ep // (4 * cores), 4, cores, tp)
    split = Mesh(mesh.devices.reshape(dims), EP_TP)
    return jax.shard_map(
        functools.partial(body, dims),
        mesh=split,
        in_specs=(
            P(EP, None),
            P(EP, "tp", None, None),
            P(EP),
            P(None, "tp"),
            P(None, "tp"),
            P(None, "tp"),
            P("tp"),
            P("tp"),
            P("tp", None),
            P(),
            P(),
            P(EP, None),
            P(None, EP_TP),
            P(None, EP_TP),
            P(EP_TP, None),
            P(None, EP),
            P(None, EP),
            P(EP, "tp"),
            P(),
            P("tp"),
        ),
        out_specs=(P(EP, "tp"), P(EP, "tp", None)),
        check_vma=False,
    )
```

```python
import functools

import jax
import jax.numpy as jnp
from jax import lax
from jax.experimental import pallas as pl
from jax.experimental.pallas import tpu as pltpu
from jax.sharding import Mesh
from jax.sharding import PartitionSpec as P

CAP = 2
CHUNKS = 2
EP = ("ep_0", "ep_1", "ep_2")
EP_TP = ("ep_0", "ep_1", "ep_2", "tp")
RESIDUAL_SCALE = 8.0**0.25
MESH = pl.DeviceIdType.MESH
F32 = jnp.float32
BF16 = jnp.bfloat16


def nt(a, b):
    return lax.dot_general(a, b, (((1,), (1,)), ((), ())), preferred_element_type=F32)


def nn(a, b):
    return jnp.dot(a, b, preferred_element_type=F32)


def iota(shape, dim):
    return lax.broadcasted_iota(jnp.int32, shape, dim)


def layer_kernel(
    dims,
    tokens_hbm,
    kv_hbm,
    lengths_hbm,
    wq_hbm,
    wk_hbm,
    wv_hbm,
    bias_hbm,
    head_gain_hbm,
    wo_hbm,
    attn_gain_hbm,
    router_hbm,
    routes_hbm,
    eg_hbm,
    eu_hbm,
    ed_hbm,
    dg_hbm,
    du_hbm,
    dd_hbm,
    mix_hbm,
    ffn_gain_hbm,
    out_ref,
    new_kv_ref,
    tok,
    kv,
    wq,
    wkv,
    wo,
    router,
    wg,
    wu,
    wd,
    dg_in,
    du_in,
    dd_in,
    dw,
    att,
    settled_cols,
    rows,
    xe,
    pb,
    pr,
    fb,
    fr,
    stats,
    lengths_ref,
    bias_ref,
    routes_ref,
    head_gain_ref,
    attn_gain_ref,
    mix_ref,
    ffn_gain_ref,
    load_sem,
    kv_sem,
    send_sem,
    recv_sem,
    hello_line,
    hello_core,
    hello_column,
    hello_x,
    hello_y,
):
    Z, X, C, Y = dims
    z, x, c, y = (lax.axis_index(a) for a in EP_TP)
    T, D = tok.shape
    DY = D // Y
    L = kv.shape[1]
    HD = kv.shape[2] // 2
    XC = X * C
    xc = x * C + c
    other = 1 - c
    sib = (z, x, other, y)

    loads = {}

    def load(name, k, src, dst):
        loads[name] = pltpu.make_async_copy(src, dst, load_sem.at[k])
        loads[name].start()

    load("tok", 0, tokens_hbm, tok)
    load("wq", 1, wq_hbm, wq)
    load("lengths", 12, lengths_hbm, lengths_ref)
    load("bias", 13, bias_hbm, bias_ref)
    load("wk", 2, wk_hbm, wkv.at[0])
    load("wv", 3, wv_hbm, wkv.at[1])
    kv_copies = [pltpu.make_async_copy(kv_hbm.at[b], kv.at[b], kv_sem.at[b]) for b in range(T)]
    for copy in kv_copies:
        copy.start()
    load("dg", 4, dg_hbm, dg_in)
    load("du", 5, du_hbm, du_in)
    load("dd", 6, dd_hbm, dd_in)
    load("wo", 7, wo_hbm, wo)
    load("router", 8, router_hbm, router)
    load("head_gain", 14, head_gain_hbm, head_gain_ref)
    load("attn_gain", 15, attn_gain_hbm, attn_gain_ref)
    load("routes", 16, routes_hbm, routes_ref)
    load("mix", 17, mix_hbm, mix_ref)
    load("ffn_gain", 18, ffn_gain_hbm, ffn_gain_ref)
    load("eg", 9, eg_hbm, wg.at[c])
    load("eu", 10, eu_hbm, wu.at[c])
    load("ed", 11, ed_hbm, wd.at[c])

    barrier = pltpu.get_barrier_semaphore()

    def tell(sem, device):
        pl.semaphore_signal(sem, inc=1, device_id=device, device_id_type=MESH)

    y_near = [(z, x, c, lax.rem(y + j, Y)) for j in sorted({1, Y - 1} - {0})]
    x_near = [(z, lax.rem(x + i, X), c, y) for i in sorted({1, X - 1} - {0})]
    for device in y_near + x_near:
        tell(barrier, device)

    def tell_later(k, _):
        tell(barrier, (k, x, c, y))
        return 0

    lax.fori_loop(z + 1, Z, tell_later, 0)

    @pl.when(c == 0)
    def _():
        tell(barrier, sib)

    plane = [(i, j) for i in range(X) for j in range(Y) if (i, j) != (0, 0)]
    plane.sort(key=lambda p: -(min(p[0], X - p[0]) + min(p[1], Y - p[1])))

    def plane_peer(i, j):
        return lax.rem(x + i, X), lax.rem(y + j, Y)

    loads["tok"].wait()
    loads["wq"].wait()
    tokens = tok[...]
    queries = nn(tokens, wq[...]).astype(BF16).astype(F32)
    lane = iota((T, 2 * HD), 1)
    turned = pltpu.roll(queries, HD, 1)
    both = jnp.concatenate(
        [jnp.where(lane < HD, queries, 0.0), jnp.where(lane < HD, turned, 0.0)], axis=0
    ).astype(BF16)
    loads["wk"].wait()
    loads["wv"].wait()
    new_kv_ref[...] = nt(tokens, wkv[...].reshape(2 * HD, D)).astype(BF16)

    loads["lengths"].wait()
    loads["bias"].wait()
    pl.semaphore_wait(barrier, len(y_near) + len(x_near) + z + c)

    def answer(k, _):
        tell(hello_line.at[z], (k, x, c, y))
        return 0

    lax.fori_loop(0, z, answer, 0)

    @pl.when(c == 1)
    def _():
        tell(hello_core, sib)

    for device in y_near:
        tell(hello_y, device)
    for device in x_near:
        tell(hello_x, device)

    R = 2 * T
    row_seq = lax.rem(iota((R, 1), 0), T)
    scores = jnp.zeros((R, L), F32)
    limit = jnp.zeros((R, 1), jnp.int32)
    for b in range(T):
        kv_copies[b].wait()
        scores = jnp.where(row_seq == b, nt(both, kv[b]), scores)
        limit = jnp.where(row_seq == b, lengths_ref[b], limit)
    bias = jnp.where(iota((R, 1), 0) < T, bias_ref[0], bias_ref[1])
    scores = scores * HD ** (-0.5) + bias
    tail = jnp.log1p(jnp.exp(-jnp.abs(scores)))
    visible = iota((R, L), 1) < limit
    survive = jnp.where(visible, jnp.minimum(-scores, 0.0) - tail, 0.0)
    taken = jnp.minimum(scores, 0.0) - tail
    blocks = L // 128
    left = jnp.concatenate([survive[:, k * 128 : (k + 1) * 128] for k in range(blocks)], axis=0)
    later = jnp.where(
        (iota((128, 256), 1) >= 128) | (iota((128, 256), 0) > iota((128, 256), 1)), 1.0, 0.0
    ).astype(BF16)
    sums = jnp.zeros((blocks * R, 256), F32)
    for _ in range(3):
        piece = left.astype(BF16)
        sums = sums + nn(piece, later)
        left = left - piece.astype(F32)
    beyond = jnp.zeros((R, 128), F32)
    parts = []
    for k in reversed(range(blocks)):
        here = slice(k * R, (k + 1) * R)
        span = slice(k * 128, (k + 1) * 128)
        parts.append(
            jnp.where(
                visible[:, span], jnp.exp(taken[:, span] + (sums[here, :128] + beyond)), 0.0
            )
        )
        beyond = beyond + sums[here, 128:]
    weights = jnp.concatenate(parts[::-1], axis=1).astype(BF16)
    blended = jnp.zeros((R, 2 * HD), F32)
    for b in range(T):
        blended = jnp.where(row_seq == b, nn(weights, kv[b]), blended)
    wide = iota((R, 2 * HD), 1)
    square = jnp.sum(jnp.where(wide >= HD, blended * blended, 0.0), axis=1, keepdims=True)
    blended = blended * lax.rsqrt(square / HD + 1e-06)
    heads = jnp.where(lane < HD, pltpu.roll(blended[:T], HD, 1), blended[T:])
    loads["head_gain"].wait()
    normed = (heads * head_gain_ref[...]).astype(BF16)
    loads["wo"].wait()
    att[y] = nn(normed, wo[...]).astype(BF16)


    def send(src, dst, k, device):
        pltpu.make_async_remote_copy(
            src_ref=src,
            dst_ref=dst,
            send_sem=send_sem.at[k],
            recv_sem=recv_sem.at[k],
            device_id=device,
            device_id_type=MESH,
        ).start()

    def arrived(ref, k):
        pltpu.make_async_copy(ref, ref, recv_sem.at[k]).wait()

    def left_here(ref, k):
        pltpu.make_async_copy(ref, ref, send_sem.at[k]).wait()

    pl.semaphore_wait(hello_y, len(y_near))
    for j in range(1, Y):
        send(att.at[y], att.at[y], 0, (z, x, c, lax.rem(y + j, Y)))
    pl.semaphore_wait(hello_x, len(x_near))
    for i in range(1, X):
        tell(hello_column, (z, lax.rem(x + i, X), c, y))
    for name in ("dg", "du", "dd"):
        loads[name].wait()
    FD = dg_in.shape[0]
    FDP = dw.shape[1]

    def padded(values):
        spare = jnp.zeros((FDP - FD, values.shape[1]), F32)
        return jnp.concatenate([values.astype(F32), spare], axis=0).astype(BF16)

    dw[xc, :, :D] = padded(dg_in[...])
    dw[xc, :, D : 2 * D] = padded(du_in[...])
    dw[xc, :, 2 * D :] = padded(dd_in[...])
    for i in range(1, X):
        send(dw.at[xc], dw.at[xc], 4, (z, lax.rem(x + i, X), c, y))
    for name in ("eg", "eu", "ed"):
        loads[name].wait()

    @pl.when(c == 0)
    def _():
        pl.semaphore_wait(hello_core, 1)

    send(wg.at[c], wg.at[c], 1, sib)
    send(wu.at[c], wu.at[c], 2, sib)
    send(wd.at[c], wd.at[c], 3, sib)
    send(dw.at[xc], dw.at[xc], 5, sib)

    for name in ("attn_gain", "router", "routes", "mix", "ffn_gain"):
        loads[name].wait()
    token_row = iota((T, 1), 0)
    routes = []
    for j in range(2):
        column = jnp.zeros((T, 1), jnp.int32)
        for t in range(T):
            column = jnp.where(token_row == t, routes_ref[j, t], column)
        routes.append(column)
    experts = router.shape[0]
    lanes = iota((T, 128), 1)
    lane_expert = lax.rem(lanes, experts)
    lane_group = lanes // experts
    hits = [lane_expert == r for r in routes]
    named = jnp.where(hits[0] | hits[1], 1.0, 0.0)
    before = jnp.zeros((T, 128), F32)
    for t in range(T - 1):
        before = before + jnp.where(token_row > t, named[t : t + 1, :], 0.0)
    lane_slot = lax.rem(lane_group, 2).astype(F32)
    placed = jnp.where(before == lane_slot, named, 0.0)
    mix_row = jnp.concatenate(
        [mix_ref[k : k + 1, :].astype(F32) for k in range(D // 128)], axis=1
    )
    arrived(att.at[pl.ds(0, Y - 1)], 0)
    attended = att[0].astype(F32)
    for j in range(1, Y):
        attended = attended + att[j].astype(F32)
    gain = jnp.concatenate([attn_gain_ref[k : k + 1, :] for k in range(D // 128)], axis=1)
    values = RESIDUAL_SCALE * tokens.astype(F32) + attended
    centred = values - jnp.mean(values, axis=1, keepdims=True)
    spread = jnp.mean(centred * centred, axis=1, keepdims=True)
    settled = (centred * lax.rsqrt(spread + 1e-05) * gain).astype(BF16)
    for j in range(Y):
        settled_cols[j] = settled[:, j * DY : (j + 1) * DY]
    logits = nt(settled, router[...])
    mix = 1.0 / (
        1.0 + jnp.exp(-jnp.sum(settled.astype(F32) * mix_row, axis=1, keepdims=True))
    )
    small = iota((T, experts), 1)
    picked = [
        jnp.sum(jnp.where(small == r, logits, 0.0), axis=1, keepdims=True) for r in routes
    ]
    share = [1.0 / (1.0 + jnp.exp(picked[1 - j] - picked[j])) for j in range(2)]
    placed_share = placed * jnp.where(hits[0], share[0], share[1])

    def high(v):
        return v.astype(BF16).astype(F32)

    share_high = high(placed_share)
    mix_high = high(mix)
    table = jnp.where(
        lane_group < 2, placed, jnp.where(lane_group < 4, share_high, placed_share - share_high)
    )
    table = jnp.where(
        lanes < 6 * experts,
        table,
        jnp.where(
            lanes == 6 * experts,
            mix_high,
            jnp.where(lanes == 6 * experts + 1, mix - mix_high, 0.0),
        ),
    )
    rows[y, z, :, DY:] = table.astype(BF16)
    rows[y, z, :, :DY] = settled_cols[y]

    def send_rows(k, _):
        send(rows.at[y, z], rows.at[y, z], 16 + z // (Z // CHUNKS), (k, x, c, y))
        return 0

    def send_rows_later(k, _):
        pl.semaphore_wait(hello_line.at[k], 1)
        return send_rows(k, 0)

    lax.fori_loop(0, z, send_rows, 0)
    lax.fori_loop(z + 1, Z, send_rows_later, 0)
    pl.semaphore_wait(hello_column, X - 1)
    arrived(dw.at[pl.ds(0, X - 1)], 4)
    for i in range(1, X):
        passed = lax.rem(x + i, X) * C + c
        send(dw.at[passed], dw.at[passed], 5, sib)

    ZC = Z // CHUNKS
    TC = ZC * T
    SC = ZC * CAP
    seat = y * X + x
    sel_row = iota((SC, 128), 0)
    sel_pick = jnp.where(
        iota((SC, 128), 1) == lax.rem(sel_row, CAP) * experts + z, 1.0, 0.0
    ).astype(BF16)
    sel_mask = iota((SC, TC), 0) // CAP == iota((SC, TC), 1) // T
    share_row = iota((3 * SC, 128), 0)
    share_group = jnp.where(share_row < 2 * SC, 2, 4) + lax.rem(share_row, CAP)
    share_pick = jnp.where(
        iota((3 * SC, 128), 1) == share_group * experts + z, 1.0, 0.0
    ).astype(BF16)
    share_mask = iota((TC, 3 * SC), 0) // T == lax.rem(iota((TC, 3 * SC), 1), SC) // CAP
    fact_lane = iota((TC, 128), 1)
    mix_lanes = (fact_lane == 6 * experts) | (fact_lane == 6 * experts + 1)
    F = 2 * wg.shape[1]
    mixing = {}

    def arrived_line(buf, g, k):
        first = g * ZC

        @pl.when(z // ZC == g)
        def _():
            if ZC > 1:
                arrived(buf.at[pl.ds(first, ZC - 1)], k)

        @pl.when(z // ZC != g)
        def _():
            arrived(buf.at[pl.ds(first, ZC)], k)

    def gather(g):
        first = g * ZC
        arrived_line(rows.at[y], g, 16 + g)
        facts = rows[y, first : first + ZC, :, DY:].astype(F32).reshape(TC, 128).astype(BF16)
        select = jnp.where(sel_mask, nt(sel_pick, facts), 0.0).astype(BF16)
        own = rows[y, first : first + ZC, :, :DY].astype(F32).reshape(TC, DY).astype(BF16)
        xe[g, seat] = nn(select, own).astype(BF16)
        for i, j in plane:
            px, py = plane_peer(i, j)
            send(xe.at[g, seat], xe.at[g, seat], 24 + g, (z, px, c, py))
        shares = jnp.where(share_mask, nt(facts, share_pick), 0.0).astype(BF16)
        mixes = jnp.sum(
            jnp.where(mix_lanes, facts.astype(F32), 0.0), axis=1, keepdims=True
        )
        mixing[g] = (shares, mixes)

    def expert(g):
        arrived(xe.at[g, pl.ds(0, X * Y - 1)], 24 + g)
        received = jnp.concatenate(
            [
                xe[g, j * X : (j + 1) * X].astype(F32).reshape(X * SC, DY).astype(BF16)
                for j in range(Y)
            ],
            axis=1,
        )
        gate_pre = nt(received, wg[...].reshape(F, D))
        up_pre = nt(received, wu[...].reshape(F, D))
        hidden = (gate_pre / (1.0 + jnp.exp(-gate_pre)) * up_pre).astype(BF16)
        partial = nn(hidden, wd[...].reshape(F, D))
        for i in range(X):
            for j in range(Y):
                pb[g, j * X + i] = partial[
                    i * SC : (i + 1) * SC, j * DY : (j + 1) * DY
                ].astype(BF16)
        for i, j in plane:
            px, py = plane_peer(i, j)
            send(pb.at[g, py * X + px], pr.at[g, seat], 32 + g, (z, px, c, py))
        pr[g, seat] = pb[g, seat]

    def stacked(a, b):
        return jnp.concatenate([dw[k, :, a:b] for k in range(XC)], axis=0)

    def dense_part(g):
        first = g * ZC
        arrived(rows.at[pl.ds(0, Y - 1), pl.ds(first, ZC), :, pl.ds(0, DY)], 28 + g)
        line = jnp.concatenate(
            [
                rows[j, first : first + ZC, :, :DY].astype(F32).reshape(TC, DY).astype(BF16)
                for j in range(Y)
            ],
            axis=1,
        )
        dense_gate = nt(line, stacked(0, D))
        dense_up = nt(line, stacked(D, 2 * D))
        dense_hidden = (dense_gate / (1.0 + jnp.exp(-dense_gate)) * dense_up).astype(BF16)
        shares, mixes = mixing[g]
        mixing[g] = (shares, nn(dense_hidden, stacked(2 * D, 2 * D + DY)) * mixes)

    def home(g):
        first = g * ZC
        arrived(pr.at[g, pl.ds(0, X * Y - 1)], 32 + g)
        served = jnp.zeros((SC, DY), F32)
        for k in range(X * Y):
            served = served + pr[g, k].astype(F32)
        served_high = served.astype(BF16)
        served_low = (served - served_high.astype(F32)).astype(BF16)
        stack = jnp.concatenate([served_high, served_low, served_high], axis=0)
        shares, dense = mixing[g]
        mixed = dense + nn(shares, stack)
        fb[first : first + ZC] = mixed.reshape(ZC, T, DY).astype(BF16)
        for to in range(first, first + ZC):

            @pl.when(z != to)
            def _(to=to):
                send(fb.at[to], fr.at[z], 10, (to, x, c, y))

            @pl.when(z == to)
            def _(to=to):
                fr[to] = fb[to]

    def spread_tokens(g):
        for j in range(1, Y):
            block = rows.at[y, pl.ds(g * ZC, ZC), :, pl.ds(0, DY)]
            send(block, block, 28 + g, (z, x, c, lax.rem(y + j, Y)))

    gather(0)
    gather(1)
    spread_tokens(0)
    arrived(wg.at[0], 1)
    arrived(wu.at[0], 2)
    arrived(wd.at[0], 3)
    expert(0)
    expert(1)
    spread_tokens(1)
    arrived(dw.at[pl.ds(0, X)], 5)
    dense_part(0)
    home(0)
    dense_part(1)
    home(1)

    arrived(fr.at[pl.ds(0, Z - 1)], 10)
    combined = RESIDUAL_SCALE * settled_cols[y].astype(F32)
    combined = combined + jnp.sum(fr[...].astype(F32), axis=0)
    centre = jnp.sum(combined, axis=1, keepdims=True) / DY
    centred = combined - centre
    scatter = jnp.sum(centred * centred, axis=1, keepdims=True)
    stats[y] = jnp.where(lanes == 0, centre, jnp.where(lanes == 1, scatter, 0.0))
    for j in range(1, Y):
        send(stats.at[y], stats.at[y], 11, (z, x, c, lax.rem(y + j, Y)))
    ffn_gain = jnp.concatenate(
        [ffn_gain_ref[k : k + 1, :] for k in range(DY // 128)], axis=1
    )
    arrived(stats.at[pl.ds(0, Y - 1)], 11)
    every = [stats[j] for j in range(Y)]
    mean = sum(e[:, 0:1] for e in every) / Y
    var = sum(e[:, 1:2] + DY * (e[:, 0:1] - mean) * (e[:, 0:1] - mean) for e in every) / D
    out_ref[...] = ((combined - mean) * lax.rsqrt(var + 1e-05) * ffn_gain).astype(BF16)

    left_here(att.at[pl.ds(0, Y - 1)], 0)
    left_here(wg.at[0], 1)
    left_here(wu.at[0], 2)
    left_here(wd.at[0], 3)
    left_here(dw.at[pl.ds(0, X - 1)], 4)
    left_here(dw.at[pl.ds(0, X)], 5)
    left_here(rows.at[y, pl.ds(0, Z - 1)], 16 + z // ZC)
    for g in range(CHUNKS):
        left_here(xe.at[g, pl.ds(0, X * Y - 1)], 24 + g)
        left_here(rows.at[pl.ds(0, Y - 1), pl.ds(g * ZC, ZC), :, pl.ds(0, DY)], 28 + g)
        left_here(pb.at[g, pl.ds(0, X * Y - 1)], 32 + g)
    left_here(fb.at[pl.ds(0, Z - 1)], 10)
    left_here(stats.at[pl.ds(0, Y - 1)], 11)


def hand_over(result_in, kv_in, result_out, kv_out, sem):
    copies = [
        pltpu.make_async_copy(result_in, result_out, sem.at[0]),
        pltpu.make_async_copy(kv_in, kv_out, sem.at[1]),
    ]
    for copy in copies:
        copy.start()
    for copy in copies:
        copy.wait()


def body(
    dims,
    tokens,
    kv_cache,
    lengths,
    w_query,
    w_key,
    w_value,
    break_bias,
    head_gain,
    w_output,
    attn_norm_gain,
    w_router,
    routes,
    expert_gate,
    expert_up,
    expert_down,
    dense_gate,
    dense_up,
    dense_down,
    mix_gate,
    ffn_norm_gain,
):
    Z, X, C, Y = dims
    T, D = tokens.shape
    DY = D // Y
    L, HD2 = kv_cache.shape[2:]
    F = expert_gate.shape[1]
    FD = dense_gate.shape[1]
    FDP = -(-FD // 8) * 8
    ZS = Z * CAP
    experts = w_router.shape[1]
    anywhere = pl.BlockSpec(memory_space=pl.ANY)
    V = pltpu.VMEM
    result, new_kv = pl.pallas_call(
        functools.partial(layer_kernel, dims),
        out_shape=(
            jax.ShapeDtypeStruct((T, DY), BF16),
            jax.ShapeDtypeStruct((T, HD2), BF16),
        ),
        in_specs=[anywhere] * 20,
        out_specs=(pl.BlockSpec(memory_space=pltpu.VMEM),) * 2,
        scratch_shapes=[
            V((T, D), BF16),
            V((T, L, HD2), BF16),
            V((D, HD2), BF16),
            V((2, HD2 // 2, D), BF16),
            V((HD2, D), BF16),
            V((experts, D), BF16),
            V((C, F, D), BF16),
            V((C, F, D), BF16),
            V((C, F, D), BF16),
            V((FD, D), BF16),
            V((FD, D), BF16),
            V((FD, DY), BF16),
            V((X * C, FDP, 2 * D + DY), BF16),
            V((Y, T, D), BF16),
            V((Y, T, DY), BF16),
            V((Y, Z, T, DY + 128), BF16),
            V((CHUNKS, X * Y, ZS // CHUNKS, DY), BF16),
            V((CHUNKS, X * Y, ZS // CHUNKS, DY), BF16),
            V((CHUNKS, X * Y, ZS // CHUNKS, DY), BF16),
            V((Z, T, DY), BF16),
            V((Z, T, DY), BF16),
            V((Y, T, 128), F32),
            pltpu.SMEM((T,), jnp.int32),
            pltpu.SMEM((2,), F32),
            pltpu.SMEM((2, T), jnp.int32),
            V((1, HD2), F32),
            V((D // 128, 128), F32),
            V((D // 128, 128), BF16),
            V((DY // 128, 128), F32),
            pltpu.SemaphoreType.DMA((19,)),
            pltpu.SemaphoreType.DMA((T,)),
            pltpu.SemaphoreType.DMA((36,)),
            pltpu.SemaphoreType.DMA((36,)),
            pltpu.SemaphoreType.REGULAR((dims[0],)),
            pltpu.SemaphoreType.REGULAR,
            pltpu.SemaphoreType.REGULAR,
            pltpu.SemaphoreType.REGULAR,
            pltpu.SemaphoreType.REGULAR,
        ],
        compiler_params=pltpu.CompilerParams(
            collective_id=0, has_side_effects=True, vmem_limit_bytes=67043328
        ),
        name="layer",
    )(
        tokens,
        kv_cache.reshape(T, L, HD2),
        lengths,
        w_query,
        w_key.T,
        w_value.T,
        break_bias,
        head_gain.reshape(1, HD2),
        w_output,
        attn_norm_gain.reshape(D // 128, 128),
        w_router.T,
        routes.T,
        expert_gate.T,
        expert_up.T,
        expert_down,
        dense_gate.T,
        dense_up.T,
        dense_down,
        mix_gate.reshape(D // 128, 128),
        ffn_norm_gain.reshape(DY // 128, 128),
    )
    result, new_kv = pl.pallas_call(
        hand_over,
        out_shape=(
            jax.ShapeDtypeStruct((T, DY), BF16),
            jax.ShapeDtypeStruct((T, HD2), BF16),
        ),
        in_specs=[anywhere] * 2,
        out_specs=(anywhere, anywhere),
        scratch_shapes=[pltpu.SemaphoreType.DMA((2,))],
        name="hand_over",
    )(result, new_kv)
    return result, new_kv.reshape(T, 1, HD2)


def solution(mesh):
    cores = 2
    ep, tp = mesh.shape["ep"], mesh.shape["tp"]
    dims = (ep // (4 * cores), 4, cores, tp)
    split = Mesh(mesh.devices.reshape(dims), EP_TP)
    return jax.shard_map(
        functools.partial(body, dims),
        mesh=split,
        in_specs=(
            P(EP, None),
            P(EP, "tp", None, None),
            P(EP),
            P(None, "tp"),
            P(None, "tp"),
            P(None, "tp"),
            P("tp"),
            P("tp"),
            P("tp", None),
            P(),
            P(),
            P(EP, None),
            P(None, EP_TP),
            P(None, EP_TP),
            P(EP_TP, None),
            P(None, EP),
            P(None, EP),
            P(EP, "tp"),
            P(),
            P("tp"),
        ),
        out_specs=(P(EP, "tp"), P(EP, "tp", None)),
        check_vma=False,
    )
```

```python
import functools

import jax
import jax.numpy as jnp
from jax import lax
from jax.experimental import pallas as pl
from jax.experimental.pallas import tpu as pltpu
from jax.sharding import Mesh
from jax.sharding import PartitionSpec as P

CAP = 2
CHUNKS = 2
EP = ("ep_0", "ep_1", "ep_2")
EP_TP = ("ep_0", "ep_1", "ep_2", "tp")
RESIDUAL_SCALE = 8.0**0.25
MESH = pl.DeviceIdType.MESH
F32 = jnp.float32
BF16 = jnp.bfloat16


def nt(a, b):
    return lax.dot_general(a, b, (((1,), (1,)), ((), ())), preferred_element_type=F32)


def nn(a, b):
    return jnp.dot(a, b, preferred_element_type=F32)


def iota(shape, dim):
    return lax.broadcasted_iota(jnp.int32, shape, dim)


def layer_kernel(
    dims,
    tokens_hbm,
    kv_hbm,
    lengths_hbm,
    wq_hbm,
    wk_hbm,
    wv_hbm,
    bias_hbm,
    head_gain_hbm,
    wo_hbm,
    attn_gain_hbm,
    router_hbm,
    routes_hbm,
    eg_hbm,
    eu_hbm,
    ed_hbm,
    dg_hbm,
    du_hbm,
    dd_hbm,
    mix_hbm,
    ffn_gain_hbm,
    out_ref,
    new_kv_ref,
    tok,
    kv,
    wq,
    wkv,
    wo,
    router,
    wg,
    wu,
    wd,
    dg_in,
    du_in,
    dd_in,
    dw,
    att,
    settled_cols,
    rows,
    xe,
    pb,
    pr,
    fb,
    fr,
    stats,
    lengths_ref,
    bias_ref,
    routes_ref,
    head_gain_ref,
    attn_gain_ref,
    mix_ref,
    ffn_gain_ref,
    load_sem,
    kv_sem,
    send_sem,
    recv_sem,
    hello_line,
    hello_core,
    hello_column,
    hello_x,
    hello_y,
):
    Z, X, C, Y = dims
    z, x, c, y = (lax.axis_index(a) for a in EP_TP)
    T, D = tok.shape
    DY = D // Y
    L = kv.shape[1]
    HD = kv.shape[2] // 2
    XC = X * C
    xc = x * C + c
    other = 1 - c
    sib = (z, x, other, y)

    loads = {}

    def load(name, k, src, dst):
        loads[name] = pltpu.make_async_copy(src, dst, load_sem.at[k])
        loads[name].start()

    load("tok", 0, tokens_hbm, tok)
    load("wq", 1, wq_hbm, wq)
    load("lengths", 12, lengths_hbm, lengths_ref)
    load("bias", 13, bias_hbm, bias_ref)
    load("wk", 2, wk_hbm, wkv.at[0])
    load("wv", 3, wv_hbm, wkv.at[1])
    kv_copies = [pltpu.make_async_copy(kv_hbm.at[b], kv.at[b], kv_sem.at[b]) for b in range(T)]
    for copy in kv_copies:
        copy.start()
    load("dg", 4, dg_hbm, dg_in)
    load("du", 5, du_hbm, du_in)
    load("dd", 6, dd_hbm, dd_in)
    load("wo", 7, wo_hbm, wo)
    load("router", 8, router_hbm, router)
    load("head_gain", 14, head_gain_hbm, head_gain_ref)
    load("attn_gain", 15, attn_gain_hbm, attn_gain_ref)
    load("routes", 16, routes_hbm, routes_ref)
    load("mix", 17, mix_hbm, mix_ref)
    load("ffn_gain", 18, ffn_gain_hbm, ffn_gain_ref)
    load("eg", 9, eg_hbm, wg.at[c])
    load("eu", 10, eu_hbm, wu.at[c])
    load("ed", 11, ed_hbm, wd.at[c])

    barrier = pltpu.get_barrier_semaphore()

    def tell(sem, device):
        pl.semaphore_signal(sem, inc=1, device_id=device, device_id_type=MESH)

    y_near = [(z, x, c, lax.rem(y + j, Y)) for j in sorted({1, Y - 1} - {0})]
    x_near = [(z, lax.rem(x + i, X), c, y) for i in sorted({1, X - 1} - {0})]
    for device in y_near + x_near:
        tell(barrier, device)

    def tell_later(k, _):
        tell(barrier, (k, x, c, y))
        return 0

    lax.fori_loop(z + 1, Z, tell_later, 0)

    @pl.when(c == 0)
    def _():
        tell(barrier, sib)

    plane = [(i, j) for i in range(X) for j in range(Y) if (i, j) != (0, 0)]
    plane.sort(key=lambda p: -(min(p[0], X - p[0]) + min(p[1], Y - p[1])))

    def plane_peer(i, j):
        return lax.rem(x + i, X), lax.rem(y + j, Y)

    loads["tok"].wait()
    loads["wq"].wait()
    tokens = tok[...]
    queries = nn(tokens, wq[...]).astype(BF16).astype(F32)
    lane = iota((T, 2 * HD), 1)
    turned = pltpu.roll(queries, HD, 1)
    both = jnp.concatenate(
        [jnp.where(lane < HD, queries, 0.0), jnp.where(lane < HD, turned, 0.0)], axis=0
    ).astype(BF16)
    loads["wk"].wait()
    loads["wv"].wait()
    new_kv_ref[...] = nt(tokens, wkv[...].reshape(2 * HD, D)).astype(BF16)

    loads["lengths"].wait()
    loads["bias"].wait()
    pl.semaphore_wait(barrier, len(y_near) + len(x_near) + z + c)

    def answer(k, _):
        tell(hello_line.at[z], (k, x, c, y))
        return 0

    lax.fori_loop(0, z, answer, 0)

    @pl.when(c == 1)
    def _():
        tell(hello_core, sib)

    for device in y_near:
        tell(hello_y, device)
    for device in x_near:
        tell(hello_x, device)

    R = 2 * T
    row_seq = lax.rem(iota((R, 1), 0), T)
    scores = jnp.zeros((R, L), F32)
    limit = jnp.zeros((R, 1), jnp.int32)
    for b in range(T):
        kv_copies[b].wait()
        scores = jnp.where(row_seq == b, nt(both, kv[b]), scores)
        limit = jnp.where(row_seq == b, lengths_ref[b], limit)
    bias = jnp.where(iota((R, 1), 0) < T, bias_ref[0], bias_ref[1])
    scores = scores * HD ** (-0.5) + bias
    tail = jnp.log1p(jnp.exp(-jnp.abs(scores)))
    visible = iota((R, L), 1) < limit
    survive = jnp.where(visible, jnp.minimum(-scores, 0.0) - tail, 0.0)
    taken = jnp.minimum(scores, 0.0) - tail
    blocks = L // 128
    left = jnp.concatenate([survive[:, k * 128 : (k + 1) * 128] for k in range(blocks)], axis=0)
    later = jnp.where(
        (iota((128, 256), 1) >= 128) | (iota((128, 256), 0) > iota((128, 256), 1)), 1.0, 0.0
    ).astype(BF16)
    sums = jnp.zeros((blocks * R, 256), F32)
    for _ in range(3):
        piece = left.astype(BF16)
        sums = sums + nn(piece, later)
        left = left - piece.astype(F32)
    beyond = jnp.zeros((R, 128), F32)
    parts = []
    for k in reversed(range(blocks)):
        here = slice(k * R, (k + 1) * R)
        span = slice(k * 128, (k + 1) * 128)
        parts.append(
            jnp.where(
                visible[:, span], jnp.exp(taken[:, span] + (sums[here, :128] + beyond)), 0.0
            )
        )
        beyond = beyond + sums[here, 128:]
    weights = jnp.concatenate(parts[::-1], axis=1).astype(BF16)
    blended = jnp.zeros((R, 2 * HD), F32)
    for b in range(T):
        blended = jnp.where(row_seq == b, nn(weights, kv[b]), blended)
    wide = iota((R, 2 * HD), 1)
    square = jnp.sum(jnp.where(wide >= HD, blended * blended, 0.0), axis=1, keepdims=True)
    blended = blended * lax.rsqrt(square / HD + 1e-06)
    heads = jnp.where(lane < HD, pltpu.roll(blended[:T], HD, 1), blended[T:])
    loads["head_gain"].wait()
    normed = (heads * head_gain_ref[...]).astype(BF16)
    loads["wo"].wait()
    att[y] = nn(normed, wo[...]).astype(BF16)


    def send(src, dst, k, device):
        pltpu.make_async_remote_copy(
            src_ref=src,
            dst_ref=dst,
            send_sem=send_sem.at[k],
            recv_sem=recv_sem.at[k],
            device_id=device,
            device_id_type=MESH,
        ).start()

    def arrived(ref, k):
        pltpu.make_async_copy(ref, ref, recv_sem.at[k]).wait()

    def left_here(ref, k):
        pltpu.make_async_copy(ref, ref, send_sem.at[k]).wait()

    pl.semaphore_wait(hello_y, len(y_near))
    for j in range(1, Y):
        send(att.at[y], att.at[y], 0, (z, x, c, lax.rem(y + j, Y)))
    pl.semaphore_wait(hello_x, len(x_near))
    for i in range(1, X):
        tell(hello_column, (z, lax.rem(x + i, X), c, y))
    for name in ("dg", "du", "dd"):
        loads[name].wait()
    FD = dg_in.shape[0]
    FDP = dw.shape[1]

    def padded(values):
        spare = jnp.zeros((FDP - FD, values.shape[1]), F32)
        return jnp.concatenate([values.astype(F32), spare], axis=0).astype(BF16)

    dw[xc, :, :D] = padded(dg_in[...])
    dw[xc, :, D : 2 * D] = padded(du_in[...])
    dw[xc, :, 2 * D :] = padded(dd_in[...])
    for i in range(1, X):
        send(dw.at[xc], dw.at[xc], 4, (z, lax.rem(x + i, X), c, y))
    for name in ("eg", "eu", "ed"):
        loads[name].wait()

    @pl.when(c == 0)
    def _():
        pl.semaphore_wait(hello_core, 1)

    send(wg.at[c], wg.at[c], 1, sib)
    send(wu.at[c], wu.at[c], 2, sib)
    send(wd.at[c], wd.at[c], 3, sib)
    send(dw.at[xc], dw.at[xc], 5, sib)

    for name in ("attn_gain", "router", "routes", "mix", "ffn_gain"):
        loads[name].wait()
    token_row = iota((T, 1), 0)
    routes = []
    for j in range(2):
        column = jnp.zeros((T, 1), jnp.int32)
        for t in range(T):
            column = jnp.where(token_row == t, routes_ref[j, t], column)
        routes.append(column)
    experts = router.shape[0]
    lanes = iota((T, 128), 1)
    lane_expert = lax.rem(lanes, experts)
    lane_group = lanes // experts
    hits = [lane_expert == r for r in routes]
    named = jnp.where(hits[0] | hits[1], 1.0, 0.0)
    before = jnp.zeros((T, 128), F32)
    for t in range(T - 1):
        before = before + jnp.where(token_row > t, named[t : t + 1, :], 0.0)
    lane_slot = lax.rem(lane_group, 2).astype(F32)
    placed = jnp.where(before == lane_slot, named, 0.0)
    mix_row = jnp.concatenate(
        [mix_ref[k : k + 1, :].astype(F32) for k in range(D // 128)], axis=1
    )
    arrived(att.at[pl.ds(0, Y - 1)], 0)
    attended = att[0].astype(F32)
    for j in range(1, Y):
        attended = attended + att[j].astype(F32)
    gain = jnp.concatenate([attn_gain_ref[k : k + 1, :] for k in range(D // 128)], axis=1)
    values = RESIDUAL_SCALE * tokens.astype(F32) + attended
    centred = values - jnp.mean(values, axis=1, keepdims=True)
    spread = jnp.mean(centred * centred, axis=1, keepdims=True)
    settled = (centred * lax.rsqrt(spread + 1e-05) * gain).astype(BF16)
    for j in range(Y):
        settled_cols[j] = settled[:, j * DY : (j + 1) * DY]
    logits = nt(settled, router[...])
    mix = 1.0 / (
        1.0 + jnp.exp(-jnp.sum(settled.astype(F32) * mix_row, axis=1, keepdims=True))
    )
    small = iota((T, experts), 1)
    picked = [
        jnp.sum(jnp.where(small == r, logits, 0.0), axis=1, keepdims=True) for r in routes
    ]
    share = [1.0 / (1.0 + jnp.exp(picked[1 - j] - picked[j])) for j in range(2)]
    placed_share = placed * jnp.where(hits[0], share[0], share[1])

    def high(v):
        return v.astype(BF16).astype(F32)

    share_high = high(placed_share)
    mix_high = high(mix)
    table = jnp.where(
        lane_group < 2, placed, jnp.where(lane_group < 4, share_high, placed_share - share_high)
    )
    table = jnp.where(
        lanes < 6 * experts,
        table,
        jnp.where(
            lanes == 6 * experts,
            mix_high,
            jnp.where(lanes == 6 * experts + 1, mix - mix_high, 0.0),
        ),
    )
    rows[y, z, :, DY:] = table.astype(BF16)
    rows[y, z, :, :DY] = settled_cols[y]

    def send_rows(k, _):
        send(rows.at[y, z], rows.at[y, z], 8 + z // (Z // CHUNKS), (k, x, c, y))
        return 0

    def send_rows_later(k, _):
        pl.semaphore_wait(hello_line.at[k], 1)
        return send_rows(k, 0)

    lax.fori_loop(0, z, send_rows, 0)
    lax.fori_loop(z + 1, Z, send_rows_later, 0)
    pl.semaphore_wait(hello_column, X - 1)
    arrived(dw.at[pl.ds(0, X - 1)], 4)
    for i in range(1, X):
        passed = lax.rem(x + i, X) * C + c
        send(dw.at[passed], dw.at[passed], 5, sib)

    ZC = Z // CHUNKS
    TC = ZC * T
    SC = ZC * CAP
    seat = y * X + x
    sel_row = iota((SC, 128), 0)
    sel_pick = jnp.where(
        iota((SC, 128), 1) == lax.rem(sel_row, CAP) * experts + z, 1.0, 0.0
    ).astype(BF16)
    sel_mask = iota((SC, TC), 0) // CAP == iota((SC, TC), 1) // T
    share_row = iota((3 * SC, 128), 0)
    share_group = jnp.where(share_row < 2 * SC, 2, 4) + lax.rem(share_row, CAP)
    share_pick = jnp.where(
        iota((3 * SC, 128), 1) == share_group * experts + z, 1.0, 0.0
    ).astype(BF16)
    share_mask = iota((TC, 3 * SC), 0) // T == lax.rem(iota((TC, 3 * SC), 1), SC) // CAP
    fact_lane = iota((TC, 128), 1)
    mix_lanes = (fact_lane == 6 * experts) | (fact_lane == 6 * experts + 1)
    F = 2 * wg.shape[1]
    mixing = {}

    def arrived_line(buf, g, k):
        first = g * ZC

        @pl.when(z // ZC == g)
        def _():
            if ZC > 1:
                arrived(buf.at[pl.ds(first, ZC - 1)], k)

        @pl.when(z // ZC != g)
        def _():
            arrived(buf.at[pl.ds(first, ZC)], k)

    def gather(g):
        first = g * ZC
        arrived_line(rows.at[y], g, 8 + g)
        facts = rows[y, first : first + ZC, :, DY:].astype(F32).reshape(TC, 128).astype(BF16)
        select = jnp.where(sel_mask, nt(sel_pick, facts), 0.0).astype(BF16)
        own = rows[y, first : first + ZC, :, :DY].astype(F32).reshape(TC, DY).astype(BF16)
        xe[g, seat] = nn(select, own).astype(BF16)
        for i, j in plane:
            px, py = plane_peer(i, j)
            send(xe.at[g, seat], xe.at[g, seat], 10 + g, (z, px, c, py))
        shares = jnp.where(share_mask, nt(facts, share_pick), 0.0).astype(BF16)
        mixes = jnp.sum(
            jnp.where(mix_lanes, facts.astype(F32), 0.0), axis=1, keepdims=True
        )
        mixing[g] = (shares, mixes)

    def expert(g):
        arrived(xe.at[g, pl.ds(0, X * Y - 1)], 10 + g)
        received = jnp.concatenate(
            [
                xe[g, j * X : (j + 1) * X].reshape(X * SC, DY)
                for j in range(Y)
            ],
            axis=1,
        )
        gate_pre = nt(received, wg[...].reshape(F, D))
        up_pre = nt(received, wu[...].reshape(F, D))
        hidden = (gate_pre / (1.0 + jnp.exp(-gate_pre)) * up_pre).astype(BF16)
        partial = nn(hidden, wd[...].reshape(F, D))
        for i in range(X):
            for j in range(Y):
                pb[g, j * X + i] = partial[
                    i * SC : (i + 1) * SC, j * DY : (j + 1) * DY
                ].astype(BF16)
        for i, j in plane:
            px, py = plane_peer(i, j)
            send(pb.at[g, py * X + px], pr.at[g, seat], 14 + g, (z, px, c, py))
        pr[g, seat] = pb[g, seat]

    def stacked(a, b):
        return jnp.concatenate([dw[k, :, a:b] for k in range(XC)], axis=0)

    def dense_part(g):
        first = g * ZC
        arrived(rows.at[pl.ds(0, Y - 1), pl.ds(first, ZC), :, pl.ds(0, DY)], 12 + g)
        line = jnp.concatenate(
            [
                rows[j, first : first + ZC, :, :DY].astype(F32).reshape(TC, DY).astype(BF16)
                for j in range(Y)
            ],
            axis=1,
        )
        dense_gate = nt(line, stacked(0, D))
        dense_up = nt(line, stacked(D, 2 * D))
        dense_hidden = (dense_gate / (1.0 + jnp.exp(-dense_gate)) * dense_up).astype(BF16)
        shares, mixes = mixing[g]
        mixing[g] = (shares, nn(dense_hidden, stacked(2 * D, 2 * D + DY)) * mixes)

    def home(g):
        first = g * ZC
        arrived(pr.at[g, pl.ds(0, X * Y - 1)], 14 + g)
        served = jnp.zeros((SC, DY), F32)
        for k in range(X * Y):
            served = served + pr[g, k].astype(F32)
        served_high = served.astype(BF16)
        served_low = (served - served_high.astype(F32)).astype(BF16)
        stack = jnp.concatenate([served_high, served_low, served_high], axis=0)
        shares, dense = mixing[g]
        mixed = dense + nn(shares, stack)
        fb[first : first + ZC] = mixed.reshape(ZC, T, DY).astype(BF16)
        for to in range(first, first + ZC):

            @pl.when(z != to)
            def _(to=to):
                send(fb.at[to], fr.at[z], 6, (to, x, c, y))

            @pl.when(z == to)
            def _(to=to):
                fr[to] = fb[to]

    def spread_tokens(g):
        for j in range(1, Y):
            block = rows.at[y, pl.ds(g * ZC, ZC), :, pl.ds(0, DY)]
            send(block, block, 12 + g, (z, x, c, lax.rem(y + j, Y)))

    gather(0)
    gather(1)
    spread_tokens(0)
    arrived(wg.at[0], 1)
    arrived(wu.at[0], 2)
    arrived(wd.at[0], 3)
    expert(0)
    expert(1)
    spread_tokens(1)
    arrived(dw.at[pl.ds(0, X)], 5)
    dense_part(0)
    home(0)
    dense_part(1)
    home(1)

    arrived(fr.at[pl.ds(0, Z - 1)], 6)
    combined = RESIDUAL_SCALE * settled_cols[y].astype(F32)
    combined = combined + jnp.sum(fr[...].astype(F32), axis=0)
    centre = jnp.sum(combined, axis=1, keepdims=True) / DY
    centred = combined - centre
    scatter = jnp.sum(centred * centred, axis=1, keepdims=True)
    stats[y] = jnp.where(lanes == 0, centre, jnp.where(lanes == 1, scatter, 0.0))
    for j in range(1, Y):
        send(stats.at[y], stats.at[y], 7, (z, x, c, lax.rem(y + j, Y)))
    ffn_gain = jnp.concatenate(
        [ffn_gain_ref[k : k + 1, :] for k in range(DY // 128)], axis=1
    )
    arrived(stats.at[pl.ds(0, Y - 1)], 7)
    every = [stats[j] for j in range(Y)]
    mean = sum(e[:, 0:1] for e in every) / Y
    var = sum(e[:, 1:2] + DY * (e[:, 0:1] - mean) * (e[:, 0:1] - mean) for e in every) / D
    out_ref[...] = ((combined - mean) * lax.rsqrt(var + 1e-05) * ffn_gain).astype(BF16)

    left_here(att.at[pl.ds(0, Y - 1)], 0)
    left_here(wg.at[0], 1)
    left_here(wu.at[0], 2)
    left_here(wd.at[0], 3)
    left_here(dw.at[pl.ds(0, X - 1)], 4)
    left_here(dw.at[pl.ds(0, X)], 5)
    left_here(rows.at[y, pl.ds(0, Z - 1)], 8 + z // ZC)
    for g in range(CHUNKS):
        left_here(xe.at[g, pl.ds(0, X * Y - 1)], 10 + g)
        left_here(rows.at[pl.ds(0, Y - 1), pl.ds(g * ZC, ZC), :, pl.ds(0, DY)], 12 + g)
        left_here(pb.at[g, pl.ds(0, X * Y - 1)], 14 + g)
    left_here(fb.at[pl.ds(0, Z - 1)], 6)
    left_here(stats.at[pl.ds(0, Y - 1)], 7)


def hand_over(result_in, kv_in, result_out, kv_out, sem):
    copies = [
        pltpu.make_async_copy(result_in, result_out, sem.at[0]),
        pltpu.make_async_copy(kv_in, kv_out, sem.at[1]),
    ]
    for copy in copies:
        copy.start()
    for copy in copies:
        copy.wait()


def body(
    dims,
    tokens,
    kv_cache,
    lengths,
    w_query,
    w_key,
    w_value,
    break_bias,
    head_gain,
    w_output,
    attn_norm_gain,
    w_router,
    routes,
    expert_gate,
    expert_up,
    expert_down,
    dense_gate,
    dense_up,
    dense_down,
    mix_gate,
    ffn_norm_gain,
):
    Z, X, C, Y = dims
    T, D = tokens.shape
    DY = D // Y
    L, HD2 = kv_cache.shape[2:]
    F = expert_gate.shape[1]
    FD = dense_gate.shape[1]
    FDP = -(-FD // 8) * 8
    ZS = Z * CAP
    experts = w_router.shape[1]
    anywhere = pl.BlockSpec(memory_space=pl.ANY)
    V = pltpu.VMEM
    result, new_kv = pl.pallas_call(
        functools.partial(layer_kernel, dims),
        out_shape=(V((T, DY), BF16), V((T, HD2), BF16)),
        in_specs=[anywhere] * 20,
        out_specs=(pl.BlockSpec(memory_space=pltpu.VMEM),) * 2,
        scratch_shapes=[
            V((T, D), BF16),
            V((T, L, HD2), BF16),
            V((D, HD2), BF16),
            V((2, HD2 // 2, D), BF16),
            V((HD2, D), BF16),
            V((experts, D), BF16),
            V((C, F, D), BF16),
            V((C, F, D), BF16),
            V((C, F, D), BF16),
            V((FD, D), BF16),
            V((FD, D), BF16),
            V((FD, DY), BF16),
            V((X * C, FDP, 2 * D + DY), BF16),
            V((Y, T, D), BF16),
            V((Y, T, DY), BF16),
            V((Y, Z, T, DY + 128), BF16),
            V((CHUNKS, X * Y, ZS // CHUNKS, DY), BF16),
            V((CHUNKS, X * Y, ZS // CHUNKS, DY), BF16),
            V((CHUNKS, X * Y, ZS // CHUNKS, DY), BF16),
            V((Z, T, DY), BF16),
            V((Z, T, DY), BF16),
            V((Y, T, 128), F32),
            pltpu.SMEM((T,), jnp.int32),
            pltpu.SMEM((2,), F32),
            pltpu.SMEM((2, T), jnp.int32),
            V((1, HD2), F32),
            V((D // 128, 128), F32),
            V((D // 128, 128), BF16),
            V((DY // 128, 128), F32),
            pltpu.SemaphoreType.DMA((19,)),
            pltpu.SemaphoreType.DMA((T,)),
            pltpu.SemaphoreType.DMA((16,)),
            pltpu.SemaphoreType.DMA((16,)),
            pltpu.SemaphoreType.REGULAR((dims[0],)),
            pltpu.SemaphoreType.REGULAR,
            pltpu.SemaphoreType.REGULAR,
            pltpu.SemaphoreType.REGULAR,
            pltpu.SemaphoreType.REGULAR,
        ],
        compiler_params=pltpu.CompilerParams(
            collective_id=0, has_side_effects=True, vmem_limit_bytes=64000000
        ),
        name="layer",
    )(
        tokens,
        kv_cache.reshape(T, L, HD2),
        lengths,
        w_query,
        w_key.T,
        w_value.T,
        break_bias,
        head_gain.reshape(1, HD2),
        w_output,
        attn_norm_gain.reshape(D // 128, 128),
        w_router.T,
        routes.T,
        expert_gate.T,
        expert_up.T,
        expert_down,
        dense_gate.T,
        dense_up.T,
        dense_down,
        mix_gate.reshape(D // 128, 128),
        ffn_norm_gain.reshape(DY // 128, 128),
    )
    result, new_kv = pl.pallas_call(
        hand_over,
        out_shape=(
            jax.ShapeDtypeStruct((T, DY), BF16),
            jax.ShapeDtypeStruct((T, HD2), BF16),
        ),
        in_specs=[pl.BlockSpec(memory_space=pltpu.VMEM)] * 2,
        out_specs=(anywhere, anywhere),
        scratch_shapes=[pltpu.SemaphoreType.DMA((2,))],
        compiler_params=pltpu.CompilerParams(vmem_limit_bytes=1024 * 1024),
        name="hand_over",
    )(result, new_kv)
    return result, new_kv.reshape(T, 1, HD2)


def solution(mesh):
    cores = 2
    ep, tp = mesh.shape["ep"], mesh.shape["tp"]
    dims = (ep // (4 * cores), 4, cores, tp)
    split = Mesh(mesh.devices.reshape(dims), EP_TP)
    return jax.shard_map(
        functools.partial(body, dims),
        mesh=split,
        in_specs=(
            P(EP, None),
            P(EP, "tp", None, None),
            P(EP),
            P(None, "tp"),
            P(None, "tp"),
            P(None, "tp"),
            P("tp"),
            P("tp"),
            P("tp", None),
            P(),
            P(),
            P(EP, None),
            P(None, EP_TP),
            P(None, EP_TP),
            P(EP_TP, None),
            P(None, EP),
            P(None, EP),
            P(EP, "tp"),
            P(),
            P("tp"),
        ),
        out_specs=(P(EP, "tp"), P(EP, "tp", None)),
        check_vma=False,
    )
```

```python
import functools

import jax
import jax.numpy as jnp
from jax import lax
from jax.experimental import pallas as pl
from jax.experimental.pallas import tpu as pltpu
from jax.sharding import Mesh
from jax.sharding import PartitionSpec as P

CAP = 2
CHUNKS = 2
EP = ("ep_0", "ep_1", "ep_2")
EP_TP = ("ep_0", "ep_1", "ep_2", "tp")
RESIDUAL_SCALE = 8.0**0.25
MESH = pl.DeviceIdType.MESH
F32 = jnp.float32
BF16 = jnp.bfloat16


def nt(a, b):
    return lax.dot_general(a, b, (((1,), (1,)), ((), ())), preferred_element_type=F32)


def nn(a, b):
    return jnp.dot(a, b, preferred_element_type=F32)


def iota(shape, dim):
    return lax.broadcasted_iota(jnp.int32, shape, dim)


def layer_kernel(
    dims,
    tokens_hbm,
    kv_hbm,
    lengths_hbm,
    wq_hbm,
    wk_hbm,
    wv_hbm,
    bias_hbm,
    head_gain_hbm,
    wo_hbm,
    attn_gain_hbm,
    router_hbm,
    routes_hbm,
    eg_hbm,
    eu_hbm,
    ed_hbm,
    dg_hbm,
    du_hbm,
    dd_hbm,
    mix_hbm,
    ffn_gain_hbm,
    out_ref,
    new_kv_ref,
    tok,
    kv,
    wq,
    wkv,
    wo,
    router,
    wg,
    wu,
    wd,
    dg_in,
    du_in,
    dd_in,
    dw,
    att,
    settled_cols,
    rows,
    xe,
    pb,
    pr,
    fb,
    fr,
    stats,
    lengths_ref,
    bias_ref,
    routes_ref,
    head_gain_ref,
    attn_gain_ref,
    mix_ref,
    ffn_gain_ref,
    load_sem,
    kv_sem,
    send_sem,
    recv_sem,
    hello_line,
    hello_core,
    hello_column,
    hello_x,
    hello_y,
):
    Z, X, C, Y = dims
    z, x, c, y = (lax.axis_index(a) for a in EP_TP)
    T, D = tok.shape
    DY = D // Y
    L = kv.shape[1]
    HD = kv.shape[2] // 2
    XC = X * C
    xc = x * C + c
    other = 1 - c
    sib = (z, x, other, y)

    loads = {}

    def load(name, k, src, dst):
        loads[name] = pltpu.make_async_copy(src, dst, load_sem.at[k])
        loads[name].start()

    load("tok", 0, tokens_hbm, tok)
    load("wq", 1, wq_hbm, wq)
    load("lengths", 12, lengths_hbm, lengths_ref)
    load("bias", 13, bias_hbm, bias_ref)
    load("wk", 2, wk_hbm, wkv.at[0])
    load("wv", 3, wv_hbm, wkv.at[1])
    kv_copies = [pltpu.make_async_copy(kv_hbm.at[b], kv.at[b], kv_sem.at[b]) for b in range(T)]
    for copy in kv_copies:
        copy.start()
    load("dg", 4, dg_hbm, dg_in)
    load("du", 5, du_hbm, du_in)
    load("dd", 6, dd_hbm, dd_in)
    load("wo", 7, wo_hbm, wo)
    load("router", 8, router_hbm, router)
    load("head_gain", 14, head_gain_hbm, head_gain_ref)
    load("attn_gain", 15, attn_gain_hbm, attn_gain_ref)
    load("routes", 16, routes_hbm, routes_ref)
    load("mix", 17, mix_hbm, mix_ref)
    load("ffn_gain", 18, ffn_gain_hbm, ffn_gain_ref)
    load("eg", 9, eg_hbm, wg.at[c])
    load("eu", 10, eu_hbm, wu.at[c])
    load("ed", 11, ed_hbm, wd.at[c])

    barrier = pltpu.get_barrier_semaphore()

    def tell(sem, device):
        pl.semaphore_signal(sem, inc=1, device_id=device, device_id_type=MESH)

    y_near = [(z, x, c, lax.rem(y + j, Y)) for j in sorted({1, Y - 1} - {0})]
    x_near = [(z, lax.rem(x + i, X), c, y) for i in sorted({1, X - 1} - {0})]
    for device in y_near + x_near:
        tell(barrier, device)

    def tell_later(k, _):
        tell(barrier, (k, x, c, y))
        return 0

    lax.fori_loop(z + 1, Z, tell_later, 0)

    @pl.when(c == 0)
    def _():
        tell(barrier, sib)

    plane = [(i, j) for i in range(X) for j in range(Y) if (i, j) != (0, 0)]
    plane.sort(key=lambda p: -(min(p[0], X - p[0]) + min(p[1], Y - p[1])))

    def plane_peer(i, j):
        return lax.rem(x + i, X), lax.rem(y + j, Y)

    loads["tok"].wait()
    loads["wq"].wait()
    tokens = tok[...]
    queries = nn(tokens, wq[...]).astype(BF16).astype(F32)
    lane = iota((T, 2 * HD), 1)
    turned = pltpu.roll(queries, HD, 1)
    both = jnp.concatenate(
        [jnp.where(lane < HD, queries, 0.0), jnp.where(lane < HD, turned, 0.0)], axis=0
    ).astype(BF16)
    loads["wk"].wait()
    loads["wv"].wait()
    new_kv_ref[...] = nt(tokens, wkv[...].reshape(2 * HD, D)).astype(BF16)

    loads["lengths"].wait()
    loads["bias"].wait()
    pl.semaphore_wait(barrier, len(y_near) + len(x_near) + z + c)

    def answer(k, _):
        tell(hello_line.at[z], (k, x, c, y))
        return 0

    lax.fori_loop(0, z, answer, 0)

    @pl.when(c == 1)
    def _():
        tell(hello_core, sib)

    for device in y_near:
        tell(hello_y, device)
    for device in x_near:
        tell(hello_x, device)

    R = 2 * T
    row_seq = lax.rem(iota((R, 1), 0), T)
    scores = jnp.zeros((R, L), F32)
    limit = jnp.zeros((R, 1), jnp.int32)
    for b in range(T):
        kv_copies[b].wait()
        scores = jnp.where(row_seq == b, nt(both, kv[b]), scores)
        limit = jnp.where(row_seq == b, lengths_ref[b], limit)
    bias = jnp.where(iota((R, 1), 0) < T, bias_ref[0], bias_ref[1])
    scores = scores * HD ** (-0.5) + bias
    tail = jnp.log1p(jnp.exp(-jnp.abs(scores)))
    visible = iota((R, L), 1) < limit
    survive = jnp.where(visible, jnp.minimum(-scores, 0.0) - tail, 0.0)
    taken = jnp.minimum(scores, 0.0) - tail
    blocks = L // 128
    left = jnp.concatenate([survive[:, k * 128 : (k + 1) * 128] for k in range(blocks)], axis=0)
    later = jnp.where(
        (iota((128, 256), 1) >= 128) | (iota((128, 256), 0) > iota((128, 256), 1)), 1.0, 0.0
    ).astype(BF16)
    sums = jnp.zeros((blocks * R, 256), F32)
    for _ in range(3):
        piece = left.astype(BF16)
        sums = sums + nn(piece, later)
        left = left - piece.astype(F32)
    beyond = jnp.zeros((R, 128), F32)
    parts = []
    for k in reversed(range(blocks)):
        here = slice(k * R, (k + 1) * R)
        span = slice(k * 128, (k + 1) * 128)
        parts.append(
            jnp.where(
                visible[:, span], jnp.exp(taken[:, span] + (sums[here, :128] + beyond)), 0.0
            )
        )
        beyond = beyond + sums[here, 128:]
    weights = jnp.concatenate(parts[::-1], axis=1).astype(BF16)
    blended = jnp.zeros((R, 2 * HD), F32)
    for b in range(T):
        blended = jnp.where(row_seq == b, nn(weights, kv[b]), blended)
    wide = iota((R, 2 * HD), 1)
    square = jnp.sum(jnp.where(wide >= HD, blended * blended, 0.0), axis=1, keepdims=True)
    blended = blended * lax.rsqrt(square / HD + 1e-06)
    heads = jnp.where(lane < HD, pltpu.roll(blended[:T], HD, 1), blended[T:])
    loads["head_gain"].wait()
    normed = (heads * head_gain_ref[...]).astype(BF16)
    loads["wo"].wait()
    att[y] = nn(normed, wo[...]).astype(BF16)


    def send(src, dst, k, device):
        pltpu.make_async_remote_copy(
            src_ref=src,
            dst_ref=dst,
            send_sem=send_sem.at[k],
            recv_sem=recv_sem.at[k],
            device_id=device,
            device_id_type=MESH,
        ).start()

    def arrived(ref, k):
        pltpu.make_async_copy(ref, ref, recv_sem.at[k]).wait()

    def left_here(ref, k):
        pltpu.make_async_copy(ref, ref, send_sem.at[k]).wait()

    pl.semaphore_wait(hello_y, len(y_near))
    for j in range(1, Y):
        send(att.at[y], att.at[y], 0, (z, x, c, lax.rem(y + j, Y)))
    pl.semaphore_wait(hello_x, len(x_near))
    for i in range(1, X):
        tell(hello_column, (z, lax.rem(x + i, X), c, y))
    for name in ("dg", "du", "dd"):
        loads[name].wait()
    FD = dg_in.shape[0]
    FDP = dw.shape[1]

    def padded(values):
        spare = jnp.zeros((FDP - FD, values.shape[1]), F32)
        return jnp.concatenate([values.astype(F32), spare], axis=0).astype(BF16)

    dw[xc, :, :D] = padded(dg_in[...])
    dw[xc, :, D : 2 * D] = padded(du_in[...])
    dw[xc, :, 2 * D :] = padded(dd_in[...])
    for i in range(1, X):
        send(dw.at[xc], dw.at[xc], 4, (z, lax.rem(x + i, X), c, y))
    for name in ("eg", "eu", "ed"):
        loads[name].wait()

    @pl.when(c == 0)
    def _():
        pl.semaphore_wait(hello_core, 1)

    send(wg.at[c], wg.at[c], 1, sib)
    send(wu.at[c], wu.at[c], 2, sib)
    send(wd.at[c], wd.at[c], 3, sib)
    send(dw.at[xc], dw.at[xc], 5, sib)

    for name in ("attn_gain", "router", "routes", "mix", "ffn_gain"):
        loads[name].wait()
    token_row = iota((T, 1), 0)
    routes = []
    for j in range(2):
        column = jnp.zeros((T, 1), jnp.int32)
        for t in range(T):
            column = jnp.where(token_row == t, routes_ref[j, t], column)
        routes.append(column)
    experts = router.shape[0]
    lanes = iota((T, 128), 1)
    lane_expert = lax.rem(lanes, experts)
    lane_group = lanes // experts
    hits = [lane_expert == r for r in routes]
    named = jnp.where(hits[0] | hits[1], 1.0, 0.0)
    before = jnp.zeros((T, 128), F32)
    for t in range(T - 1):
        before = before + jnp.where(token_row > t, named[t : t + 1, :], 0.0)
    lane_slot = lax.rem(lane_group, 2).astype(F32)
    placed = jnp.where(before == lane_slot, named, 0.0)
    mix_row = jnp.concatenate(
        [mix_ref[k : k + 1, :].astype(F32) for k in range(D // 128)], axis=1
    )
    arrived(att.at[pl.ds(0, Y - 1)], 0)
    attended = att[0].astype(F32)
    for j in range(1, Y):
        attended = attended + att[j].astype(F32)
    gain = jnp.concatenate([attn_gain_ref[k : k + 1, :] for k in range(D // 128)], axis=1)
    values = RESIDUAL_SCALE * tokens.astype(F32) + attended
    centred = values - jnp.mean(values, axis=1, keepdims=True)
    spread = jnp.mean(centred * centred, axis=1, keepdims=True)
    settled = (centred * lax.rsqrt(spread + 1e-05) * gain).astype(BF16)
    for j in range(Y):
        settled_cols[j] = settled[:, j * DY : (j + 1) * DY]
    logits = nt(settled, router[...])
    mix = 1.0 / (
        1.0 + jnp.exp(-jnp.sum(settled.astype(F32) * mix_row, axis=1, keepdims=True))
    )
    small = iota((T, experts), 1)
    picked = [
        jnp.sum(jnp.where(small == r, logits, 0.0), axis=1, keepdims=True) for r in routes
    ]
    share = [1.0 / (1.0 + jnp.exp(picked[1 - j] - picked[j])) for j in range(2)]
    placed_share = placed * jnp.where(hits[0], share[0], share[1])

    def high(v):
        return v.astype(BF16).astype(F32)

    share_high = high(placed_share)
    mix_high = high(mix)
    table = jnp.where(
        lane_group < 2, placed, jnp.where(lane_group < 4, share_high, placed_share - share_high)
    )
    table = jnp.where(
        lanes < 6 * experts,
        table,
        jnp.where(
            lanes == 6 * experts,
            mix_high,
            jnp.where(lanes == 6 * experts + 1, mix - mix_high, 0.0),
        ),
    )
    rows[y, z, :, DY:] = table.astype(BF16)
    rows[y, z, :, :DY] = settled_cols[y]

    def send_rows(k, _):
        send(rows.at[y, z], rows.at[y, z], 8 + z // (Z // CHUNKS), (k, x, c, y))
        return 0

    def send_rows_later(k, _):
        pl.semaphore_wait(hello_line.at[k], 1)
        return send_rows(k, 0)

    lax.fori_loop(0, z, send_rows, 0)
    lax.fori_loop(z + 1, Z, send_rows_later, 0)
    pl.semaphore_wait(hello_column, X - 1)
    arrived(dw.at[pl.ds(0, X - 1)], 4)
    for i in range(1, X):
        passed = lax.rem(x + i, X) * C + c
        send(dw.at[passed], dw.at[passed], 5, sib)

    ZC = Z // CHUNKS
    TC = ZC * T
    SC = ZC * CAP
    seat = y * X + x
    sel_row = iota((SC, 128), 0)
    sel_pick = jnp.where(
        iota((SC, 128), 1) == lax.rem(sel_row, CAP) * experts + z, 1.0, 0.0
    ).astype(BF16)
    sel_mask = iota((SC, TC), 0) // CAP == iota((SC, TC), 1) // T
    share_row = iota((3 * SC, 128), 0)
    share_group = jnp.where(share_row < 2 * SC, 2, 4) + lax.rem(share_row, CAP)
    share_pick = jnp.where(
        iota((3 * SC, 128), 1) == share_group * experts + z, 1.0, 0.0
    ).astype(BF16)
    share_mask = iota((TC, 3 * SC), 0) // T == lax.rem(iota((TC, 3 * SC), 1), SC) // CAP
    fact_lane = iota((TC, 128), 1)
    mix_lanes = (fact_lane == 6 * experts) | (fact_lane == 6 * experts + 1)
    F = 2 * wg.shape[1]
    mixing = {}

    def arrived_line(buf, g, k):
        first = g * ZC

        @pl.when(z // ZC == g)
        def _():
            if ZC > 1:
                arrived(buf.at[pl.ds(first, ZC - 1)], k)

        @pl.when(z // ZC != g)
        def _():
            arrived(buf.at[pl.ds(first, ZC)], k)

    def gather(g):
        first = g * ZC
        arrived_line(rows.at[y], g, 8 + g)
        facts = rows[y, first : first + ZC, :, DY:].astype(F32).reshape(TC, 128).astype(BF16)
        select = jnp.where(sel_mask, nt(sel_pick, facts), 0.0).astype(BF16)
        own = rows[y, first : first + ZC, :, :DY].astype(F32).reshape(TC, DY).astype(BF16)
        xe[g, seat] = nn(select, own).astype(BF16)
        for i, j in plane:
            px, py = plane_peer(i, j)
            send(xe.at[g, seat], xe.at[g, seat], 10 + g, (z, px, c, py))

    def expert(g):
        arrived(xe.at[g, pl.ds(0, X * Y - 1)], 10 + g)
        received = jnp.concatenate(
            [
                xe[g, j * X : (j + 1) * X].reshape(X * SC, DY)
                for j in range(Y)
            ],
            axis=1,
        )
        gate_pre = nt(received, wg[...].reshape(F, D))
        up_pre = nt(received, wu[...].reshape(F, D))
        hidden = (gate_pre / (1.0 + jnp.exp(-gate_pre)) * up_pre).astype(BF16)
        partial = nn(hidden, wd[...].reshape(F, D))
        for i in range(X):
            for j in range(Y):
                pb[g, j * X + i] = partial[
                    i * SC : (i + 1) * SC, j * DY : (j + 1) * DY
                ].astype(BF16)
        for i, j in plane:
            px, py = plane_peer(i, j)
            send(pb.at[g, py * X + px], pr.at[g, seat], 14 + g, (z, px, c, py))
        pr[g, seat] = pb[g, seat]

    def stacked(a, b):
        return jnp.concatenate([dw[k, :, a:b] for k in range(XC)], axis=0)

    def dense_part(g):
        first = g * ZC
        arrived(rows.at[pl.ds(0, Y - 1), pl.ds(first, ZC), :, pl.ds(0, DY)], 12 + g)
        line = jnp.concatenate(
            [
                rows[j, first : first + ZC, :, :DY].astype(F32).reshape(TC, DY).astype(BF16)
                for j in range(Y)
            ],
            axis=1,
        )
        dense_gate = nt(line, stacked(0, D))
        dense_up = nt(line, stacked(D, 2 * D))
        dense_hidden = (dense_gate / (1.0 + jnp.exp(-dense_gate)) * dense_up).astype(BF16)
        facts = rows[y, first : first + ZC, :, DY:].astype(F32).reshape(TC, 128).astype(BF16)
        shares = jnp.where(share_mask, nt(facts, share_pick), 0.0).astype(BF16)
        mixes = jnp.sum(
            jnp.where(mix_lanes, facts.astype(F32), 0.0), axis=1, keepdims=True
        )
        mixing[g] = (shares, nn(dense_hidden, stacked(2 * D, 2 * D + DY)) * mixes)

    def home(g):
        first = g * ZC
        arrived(pr.at[g, pl.ds(0, X * Y - 1)], 14 + g)
        served = jnp.zeros((SC, DY), F32)
        for k in range(X * Y):
            served = served + pr[g, k].astype(F32)
        served_high = served.astype(BF16)
        served_low = (served - served_high.astype(F32)).astype(BF16)
        stack = jnp.concatenate([served_high, served_low, served_high], axis=0)
        shares, dense = mixing[g]
        mixed = dense + nn(shares, stack)
        fb[first : first + ZC] = mixed.reshape(ZC, T, DY).astype(BF16)
        for to in range(first, first + ZC):

            @pl.when(z != to)
            def _(to=to):
                send(fb.at[to], fr.at[z], 6, (to, x, c, y))

            @pl.when(z == to)
            def _(to=to):
                fr[to] = fb[to]

    def spread_tokens(g):
        for j in range(1, Y):
            block = rows.at[y, pl.ds(g * ZC, ZC), :, pl.ds(0, DY)]
            send(block, block, 12 + g, (z, x, c, lax.rem(y + j, Y)))

    early = z < Z // 2
    gather(0)

    @pl.when(jnp.logical_not(early))
    def _():
        gather(1)

    spread_tokens(0)
    arrived(wg.at[0], 1)
    arrived(wu.at[0], 2)
    arrived(wd.at[0], 3)
    expert(0)

    @pl.when(early)
    def _():
        gather(1)
        spread_tokens(1)

    @pl.when(jnp.logical_not(early))
    def _():
        expert(1)
        spread_tokens(1)

    arrived(dw.at[pl.ds(0, X)], 5)
    dense_part(0)
    home(0)

    @pl.when(early)
    def _():
        expert(1)

    dense_part(1)
    home(1)

    arrived(fr.at[pl.ds(0, Z - 1)], 6)
    combined = RESIDUAL_SCALE * settled_cols[y].astype(F32)
    combined = combined + jnp.sum(fr[...].astype(F32), axis=0)
    centre = jnp.sum(combined, axis=1, keepdims=True) / DY
    centred = combined - centre
    scatter = jnp.sum(centred * centred, axis=1, keepdims=True)
    stats[y] = jnp.where(lanes == 0, centre, jnp.where(lanes == 1, scatter, 0.0))
    for j in range(1, Y):
        send(stats.at[y], stats.at[y], 7, (z, x, c, lax.rem(y + j, Y)))
    ffn_gain = jnp.concatenate(
        [ffn_gain_ref[k : k + 1, :] for k in range(DY // 128)], axis=1
    )
    arrived(stats.at[pl.ds(0, Y - 1)], 7)
    every = [stats[j] for j in range(Y)]
    mean = sum(e[:, 0:1] for e in every) / Y
    var = sum(e[:, 1:2] + DY * (e[:, 0:1] - mean) * (e[:, 0:1] - mean) for e in every) / D
    out_ref[...] = ((combined - mean) * lax.rsqrt(var + 1e-05) * ffn_gain).astype(BF16)

    left_here(att.at[pl.ds(0, Y - 1)], 0)
    left_here(wg.at[0], 1)
    left_here(wu.at[0], 2)
    left_here(wd.at[0], 3)
    left_here(dw.at[pl.ds(0, X - 1)], 4)
    left_here(dw.at[pl.ds(0, X)], 5)
    left_here(rows.at[y, pl.ds(0, Z - 1)], 8 + z // ZC)
    for g in range(CHUNKS):
        left_here(xe.at[g, pl.ds(0, X * Y - 1)], 10 + g)
        left_here(rows.at[pl.ds(0, Y - 1), pl.ds(g * ZC, ZC), :, pl.ds(0, DY)], 12 + g)
        left_here(pb.at[g, pl.ds(0, X * Y - 1)], 14 + g)
    left_here(fb.at[pl.ds(0, Z - 1)], 6)
    left_here(stats.at[pl.ds(0, Y - 1)], 7)


def hand_over(result_in, kv_in, result_out, kv_out, sem):
    copies = [
        pltpu.make_async_copy(result_in, result_out, sem.at[0]),
        pltpu.make_async_copy(kv_in, kv_out, sem.at[1]),
    ]
    for copy in copies:
        copy.start()
    for copy in copies:
        copy.wait()


def body(
    dims,
    tokens,
    kv_cache,
    lengths,
    w_query,
    w_key,
    w_value,
    break_bias,
    head_gain,
    w_output,
    attn_norm_gain,
    w_router,
    routes,
    expert_gate,
    expert_up,
    expert_down,
    dense_gate,
    dense_up,
    dense_down,
    mix_gate,
    ffn_norm_gain,
):
    Z, X, C, Y = dims
    T, D = tokens.shape
    DY = D // Y
    L, HD2 = kv_cache.shape[2:]
    F = expert_gate.shape[1]
    FD = dense_gate.shape[1]
    FDP = -(-FD // 8) * 8
    ZS = Z * CAP
    experts = w_router.shape[1]
    anywhere = pl.BlockSpec(memory_space=pl.ANY)
    V = pltpu.VMEM
    result, new_kv = pl.pallas_call(
        functools.partial(layer_kernel, dims),
        out_shape=(V((T, DY), BF16), V((T, HD2), BF16)),
        in_specs=[anywhere] * 20,
        out_specs=(pl.BlockSpec(memory_space=pltpu.VMEM),) * 2,
        scratch_shapes=[
            V((T, D), BF16),
            V((T, L, HD2), BF16),
            V((D, HD2), BF16),
            V((2, HD2 // 2, D), BF16),
            V((HD2, D), BF16),
            V((experts, D), BF16),
            V((C, F, D), BF16),
            V((C, F, D), BF16),
            V((C, F, D), BF16),
            V((FD, D), BF16),
            V((FD, D), BF16),
            V((FD, DY), BF16),
            V((X * C, FDP, 2 * D + DY), BF16),
            V((Y, T, D), BF16),
            V((Y, T, DY), BF16),
            V((Y, Z, T, DY + 128), BF16),
            V((CHUNKS, X * Y, ZS // CHUNKS, DY), BF16),
            V((CHUNKS, X * Y, ZS // CHUNKS, DY), BF16),
            V((CHUNKS, X * Y, ZS // CHUNKS, DY), BF16),
            V((Z, T, DY), BF16),
            V((Z, T, DY), BF16),
            V((Y, T, 128), F32),
            pltpu.SMEM((T,), jnp.int32),
            pltpu.SMEM((2,), F32),
            pltpu.SMEM((2, T), jnp.int32),
            V((1, HD2), F32),
            V((D // 128, 128), F32),
            V((D // 128, 128), BF16),
            V((DY // 128, 128), F32),
            pltpu.SemaphoreType.DMA((19,)),
            pltpu.SemaphoreType.DMA((T,)),
            pltpu.SemaphoreType.DMA((16,)),
            pltpu.SemaphoreType.DMA((16,)),
            pltpu.SemaphoreType.REGULAR((dims[0],)),
            pltpu.SemaphoreType.REGULAR,
            pltpu.SemaphoreType.REGULAR,
            pltpu.SemaphoreType.REGULAR,
            pltpu.SemaphoreType.REGULAR,
        ],
        compiler_params=pltpu.CompilerParams(
            collective_id=0, has_side_effects=True, vmem_limit_bytes=64000000
        ),
        name="layer",
    )(
        tokens,
        kv_cache.reshape(T, L, HD2),
        lengths,
        w_query,
        w_key.T,
        w_value.T,
        break_bias,
        head_gain.reshape(1, HD2),
        w_output,
        attn_norm_gain.reshape(D // 128, 128),
        w_router.T,
        routes.T,
        expert_gate.T,
        expert_up.T,
        expert_down,
        dense_gate.T,
        dense_up.T,
        dense_down,
        mix_gate.reshape(D // 128, 128),
        ffn_norm_gain.reshape(DY // 128, 128),
    )
    result, new_kv = pl.pallas_call(
        hand_over,
        out_shape=(
            jax.ShapeDtypeStruct((T, DY), BF16),
            jax.ShapeDtypeStruct((T, HD2), BF16),
        ),
        in_specs=[pl.BlockSpec(memory_space=pltpu.VMEM)] * 2,
        out_specs=(anywhere, anywhere),
        scratch_shapes=[pltpu.SemaphoreType.DMA((2,))],
        compiler_params=pltpu.CompilerParams(vmem_limit_bytes=1024 * 1024),
        name="hand_over",
    )(result, new_kv)
    return result, new_kv.reshape(T, 1, HD2)


def solution(mesh):
    cores = 2
    ep, tp = mesh.shape["ep"], mesh.shape["tp"]
    dims = (ep // (4 * cores), 4, cores, tp)
    split = Mesh(mesh.devices.reshape(dims), EP_TP)
    return jax.shard_map(
        functools.partial(body, dims),
        mesh=split,
        in_specs=(
            P(EP, None),
            P(EP, "tp", None, None),
            P(EP),
            P(None, "tp"),
            P(None, "tp"),
            P(None, "tp"),
            P("tp"),
            P("tp"),
            P("tp", None),
            P(),
            P(),
            P(EP, None),
            P(None, EP_TP),
            P(None, EP_TP),
            P(EP_TP, None),
            P(None, EP),
            P(None, EP),
            P(EP, "tp"),
            P(),
            P("tp"),
        ),
        out_specs=(P(EP, "tp"), P(EP, "tp", None)),
        check_vma=False,
    )
```

```python
import functools

import jax
import jax.numpy as jnp
from jax import lax
from jax.experimental import pallas as pl
from jax.experimental.pallas import tpu as pltpu
from jax.sharding import Mesh
from jax.sharding import PartitionSpec as P

CAP = 2
CHUNKS = 2
EP = ("ep_0", "ep_1", "ep_2")
EP_TP = ("ep_0", "ep_1", "ep_2", "tp")
RESIDUAL_SCALE = 8.0**0.25
MESH = pl.DeviceIdType.MESH
F32 = jnp.float32
BF16 = jnp.bfloat16


def nt(a, b):
    return lax.dot_general(a, b, (((1,), (1,)), ((), ())), preferred_element_type=F32)


def nn(a, b):
    return jnp.dot(a, b, preferred_element_type=F32)


def iota(shape, dim):
    return lax.broadcasted_iota(jnp.int32, shape, dim)


def layer_kernel(
    dims,
    tokens_hbm,
    kv_hbm,
    lengths_hbm,
    wq_hbm,
    wk_hbm,
    wv_hbm,
    bias_hbm,
    head_gain_hbm,
    wo_hbm,
    attn_gain_hbm,
    router_hbm,
    routes_hbm,
    eg_hbm,
    eu_hbm,
    ed_hbm,
    dg_hbm,
    du_hbm,
    dd_hbm,
    mix_hbm,
    ffn_gain_hbm,
    out_ref,
    new_kv_ref,
    tok,
    kv,
    wq,
    wkv,
    wo,
    router,
    we,
    dg_in,
    du_in,
    dd_in,
    dw,
    att,
    settled_cols,
    rows,
    xe,
    pb,
    pr,
    fb,
    fr,
    stats,
    lengths_ref,
    bias_ref,
    routes_ref,
    head_gain_ref,
    attn_gain_ref,
    mix_ref,
    ffn_gain_ref,
    load_sem,
    send_sem,
    recv_sem,
    hello_line,
    hello_core,
    hello_column,
    hello_x,
    hello_y,
):
    Z, X, C, Y = dims
    z, x, c, y = (lax.axis_index(a) for a in EP_TP)
    T, D = tok.shape
    DY = D // Y
    L = kv.shape[1]
    HD = kv.shape[2] // 2
    XC = X * C
    xc = x * C + c
    other = 1 - c
    sib = (z, x, other, y)

    loads = {}

    def load(name, k, src, dst):
        loads[name] = pltpu.make_async_copy(src, dst, load_sem.at[k])
        loads[name].start()

    load("tok", 0, tokens_hbm, tok)
    load("wq", 1, wq_hbm, wq)
    load("lengths", 10, lengths_hbm, lengths_ref)
    load("bias", 11, bias_hbm, bias_ref)
    load("wk", 2, wk_hbm, wkv.at[0])
    load("wv", 2, wv_hbm, wkv.at[1])
    load("kv", 3, kv_hbm, kv)
    load("dg", 4, dg_hbm, dg_in)
    load("du", 5, du_hbm, du_in)
    load("dd", 6, dd_hbm, dd_in)
    load("wo", 7, wo_hbm, wo)
    load("router", 8, router_hbm, router)
    load("head_gain", 12, head_gain_hbm, head_gain_ref)
    load("attn_gain", 13, attn_gain_hbm, attn_gain_ref)
    load("routes", 14, routes_hbm, routes_ref)
    load("mix", 15, mix_hbm, mix_ref)
    load("ffn_gain", 16, ffn_gain_hbm, ffn_gain_ref)
    load("eg", 9, eg_hbm, we.at[c, 0])
    load("eu", 9, eu_hbm, we.at[c, 1])
    load("ed", 9, ed_hbm, we.at[c, 2])

    barrier = pltpu.get_barrier_semaphore()

    def tell(sem, device):
        pl.semaphore_signal(sem, inc=1, device_id=device, device_id_type=MESH)

    y_near = [(z, x, c, lax.rem(y + j, Y)) for j in sorted({1, Y - 1} - {0})]
    x_near = [(z, lax.rem(x + i, X), c, y) for i in sorted({1, X - 1} - {0})]
    for device in y_near + x_near:
        tell(barrier, device)

    def tell_later(k, _):
        tell(barrier, (k, x, c, y))
        return 0

    lax.fori_loop(z + 1, Z, tell_later, 0)

    @pl.when(c == 0)
    def _():
        tell(barrier, sib)

    plane = [(i, j) for i in range(X) for j in range(Y) if (i, j) != (0, 0)]
    plane.sort(key=lambda p: -(min(p[0], X - p[0]) + min(p[1], Y - p[1])))

    def plane_peer(i, j):
        return lax.rem(x + i, X), lax.rem(y + j, Y)

    loads["tok"].wait()
    loads["wq"].wait()
    tokens = tok[...]
    queries = nn(tokens, wq[...]).astype(BF16).astype(F32)
    lane = iota((T, 2 * HD), 1)
    turned = pltpu.roll(queries, HD, 1)
    both = jnp.concatenate(
        [jnp.where(lane < HD, queries, 0.0), jnp.where(lane < HD, turned, 0.0)], axis=0
    ).astype(BF16)
    pltpu.make_async_copy(wkv, wkv, load_sem.at[2]).wait()
    new_kv_ref[...] = nt(tokens, wkv[...].reshape(2 * HD, D)).astype(BF16)

    loads["lengths"].wait()
    loads["bias"].wait()
    pl.semaphore_wait(barrier, len(y_near) + len(x_near) + z + c)

    def answer(k, _):
        tell(hello_line.at[z], (k, x, c, y))
        return 0

    lax.fori_loop(0, z, answer, 0)

    @pl.when(c == 1)
    def _():
        tell(hello_core, sib)

    for device in y_near:
        tell(hello_y, device)
    for device in x_near:
        tell(hello_x, device)

    R = 2 * T
    row_seq = lax.rem(iota((R, 1), 0), T)
    scores = jnp.zeros((R, L), F32)
    limit = jnp.zeros((R, 1), jnp.int32)
    loads["kv"].wait()
    for b in range(T):
        scores = jnp.where(row_seq == b, nt(both, kv[b]), scores)
        limit = jnp.where(row_seq == b, lengths_ref[b], limit)
    bias = jnp.where(iota((R, 1), 0) < T, bias_ref[0], bias_ref[1])
    scores = scores * HD ** (-0.5) + bias
    tail = jnp.log1p(jnp.exp(-jnp.abs(scores)))
    visible = iota((R, L), 1) < limit
    survive = jnp.where(visible, jnp.minimum(-scores, 0.0) - tail, 0.0)
    taken = jnp.minimum(scores, 0.0) - tail
    blocks = L // 128
    left = jnp.concatenate([survive[:, k * 128 : (k + 1) * 128] for k in range(blocks)], axis=0)
    later = jnp.where(
        (iota((128, 256), 1) >= 128) | (iota((128, 256), 0) > iota((128, 256), 1)), 1.0, 0.0
    ).astype(BF16)
    sums = jnp.zeros((blocks * R, 256), F32)
    for _ in range(3):
        piece = left.astype(BF16)
        sums = sums + nn(piece, later)
        left = left - piece.astype(F32)
    beyond = jnp.zeros((R, 128), F32)
    parts = []
    for k in reversed(range(blocks)):
        here = slice(k * R, (k + 1) * R)
        span = slice(k * 128, (k + 1) * 128)
        parts.append(
            jnp.where(
                visible[:, span], jnp.exp(taken[:, span] + (sums[here, :128] + beyond)), 0.0
            )
        )
        beyond = beyond + sums[here, 128:]
    weights = jnp.concatenate(parts[::-1], axis=1).astype(BF16)
    blended = jnp.zeros((R, 2 * HD), F32)
    for b in range(T):
        blended = jnp.where(row_seq == b, nn(weights, kv[b]), blended)
    wide = iota((R, 2 * HD), 1)
    square = jnp.sum(jnp.where(wide >= HD, blended * blended, 0.0), axis=1, keepdims=True)
    blended = blended * lax.rsqrt(square / HD + 1e-06)
    heads = jnp.where(lane < HD, pltpu.roll(blended[:T], HD, 1), blended[T:])
    loads["head_gain"].wait()
    normed = (heads * head_gain_ref[...]).astype(BF16)
    loads["wo"].wait()
    att[y] = nn(normed, wo[...]).astype(BF16)


    def send(src, dst, k, device):
        pltpu.make_async_remote_copy(
            src_ref=src,
            dst_ref=dst,
            send_sem=send_sem.at[k],
            recv_sem=recv_sem.at[k],
            device_id=device,
            device_id_type=MESH,
        ).start()

    def arrived(ref, k):
        pltpu.make_async_copy(ref, ref, recv_sem.at[k]).wait()

    def left_here(ref, k):
        pltpu.make_async_copy(ref, ref, send_sem.at[k]).wait()

    pl.semaphore_wait(hello_y, len(y_near))
    for j in range(1, Y):
        send(att.at[y], att.at[y], 0, (z, x, c, lax.rem(y + j, Y)))
    pl.semaphore_wait(hello_x, len(x_near))
    for i in range(1, X):
        tell(hello_column, (z, lax.rem(x + i, X), c, y))
    for name in ("dg", "du", "dd"):
        loads[name].wait()
    FD = dg_in.shape[0]
    FDP = dw.shape[1]

    def padded(values):
        spare = jnp.zeros((FDP - FD, values.shape[1]), F32)
        return jnp.concatenate([values.astype(F32), spare], axis=0).astype(BF16)

    dw[xc, :, :D] = padded(dg_in[...])
    dw[xc, :, D : 2 * D] = padded(du_in[...])
    dw[xc, :, 2 * D :] = padded(dd_in[...])
    for i in range(1, X):
        send(dw.at[xc], dw.at[xc], 4, (z, lax.rem(x + i, X), c, y))
    pltpu.make_async_copy(we.at[c], we.at[c], load_sem.at[9]).wait()

    @pl.when(c == 0)
    def _():
        pl.semaphore_wait(hello_core, 1)

    send(we.at[c], we.at[c], 1, sib)
    send(dw.at[xc], dw.at[xc], 5, sib)

    for name in ("attn_gain", "router", "routes", "mix", "ffn_gain"):
        loads[name].wait()
    token_row = iota((T, 1), 0)
    routes = []
    for j in range(2):
        column = jnp.zeros((T, 1), jnp.int32)
        for t in range(T):
            column = jnp.where(token_row == t, routes_ref[j, t], column)
        routes.append(column)
    experts = router.shape[0]
    lanes = iota((T, 128), 1)
    lane_expert = lax.rem(lanes, experts)
    lane_group = lanes // experts
    hits = [lane_expert == r for r in routes]
    named = jnp.where(hits[0] | hits[1], 1.0, 0.0)
    before = jnp.zeros((T, 128), F32)
    for t in range(T - 1):
        before = before + jnp.where(token_row > t, named[t : t + 1, :], 0.0)
    lane_slot = lax.rem(lane_group, 2).astype(F32)
    placed = jnp.where(before == lane_slot, named, 0.0)
    mix_row = jnp.concatenate(
        [mix_ref[k : k + 1, :].astype(F32) for k in range(D // 128)], axis=1
    )
    arrived(att.at[pl.ds(0, Y - 1)], 0)
    attended = att[0].astype(F32)
    for j in range(1, Y):
        attended = attended + att[j].astype(F32)
    gain = jnp.concatenate([attn_gain_ref[k : k + 1, :] for k in range(D // 128)], axis=1)
    values = RESIDUAL_SCALE * tokens.astype(F32) + attended
    centred = values - jnp.mean(values, axis=1, keepdims=True)
    spread = jnp.mean(centred * centred, axis=1, keepdims=True)
    settled = (centred * lax.rsqrt(spread + 1e-05) * gain).astype(BF16)
    for j in range(Y):
        settled_cols[j] = settled[:, j * DY : (j + 1) * DY]
    logits = nt(settled, router[...])
    mix = 1.0 / (
        1.0 + jnp.exp(-jnp.sum(settled.astype(F32) * mix_row, axis=1, keepdims=True))
    )
    small = iota((T, experts), 1)
    picked = [
        jnp.sum(jnp.where(small == r, logits, 0.0), axis=1, keepdims=True) for r in routes
    ]
    share = [1.0 / (1.0 + jnp.exp(picked[1 - j] - picked[j])) for j in range(2)]
    placed_share = placed * jnp.where(hits[0], share[0], share[1])

    def high(v):
        return v.astype(BF16).astype(F32)

    share_high = high(placed_share)
    mix_high = high(mix)
    table = jnp.where(
        lane_group < 2, placed, jnp.where(lane_group < 4, share_high, placed_share - share_high)
    )
    table = jnp.where(
        lanes < 6 * experts,
        table,
        jnp.where(
            lanes == 6 * experts,
            mix_high,
            jnp.where(lanes == 6 * experts + 1, mix - mix_high, 0.0),
        ),
    )
    rows[y, z, :, DY:] = table.astype(BF16)
    rows[y, z, :, :DY] = settled_cols[y]

    def send_rows(k, _):
        send(rows.at[y, z], rows.at[y, z], 8 + z // (Z // CHUNKS), (k, x, c, y))
        return 0

    def send_rows_later(k, _):
        pl.semaphore_wait(hello_line.at[k], 1)
        return send_rows(k, 0)

    lax.fori_loop(0, z, send_rows, 0)
    lax.fori_loop(z + 1, Z, send_rows_later, 0)
    pl.semaphore_wait(hello_column, X - 1)
    arrived(dw.at[pl.ds(0, X - 1)], 4)
    for i in range(1, X):
        passed = lax.rem(x + i, X) * C + c
        send(dw.at[passed], dw.at[passed], 5, sib)

    ZC = Z // CHUNKS
    TC = ZC * T
    SC = ZC * CAP
    seat = y * X + x
    sel_row = iota((SC, 128), 0)
    sel_pick = jnp.where(
        iota((SC, 128), 1) == lax.rem(sel_row, CAP) * experts + z, 1.0, 0.0
    ).astype(BF16)
    sel_mask = iota((SC, TC), 0) // CAP == iota((SC, TC), 1) // T
    share_row = iota((3 * SC, 128), 0)
    share_group = jnp.where(share_row < 2 * SC, 2, 4) + lax.rem(share_row, CAP)
    share_pick = jnp.where(
        iota((3 * SC, 128), 1) == share_group * experts + z, 1.0, 0.0
    ).astype(BF16)
    share_mask = iota((TC, 3 * SC), 0) // T == lax.rem(iota((TC, 3 * SC), 1), SC) // CAP
    fact_lane = iota((TC, 128), 1)
    mix_lanes = (fact_lane == 6 * experts) | (fact_lane == 6 * experts + 1)
    F = C * we.shape[2]
    mixing = {}

    def arrived_line(buf, g, k):
        first = g * ZC

        @pl.when(z // ZC == g)
        def _():
            if ZC > 1:
                arrived(buf.at[pl.ds(first, ZC - 1)], k)

        @pl.when(z // ZC != g)
        def _():
            arrived(buf.at[pl.ds(first, ZC)], k)

    def gather(g):
        first = g * ZC
        arrived_line(rows.at[y], g, 8 + g)
        facts = rows[y, first : first + ZC, :, DY:].astype(F32).reshape(TC, 128).astype(BF16)
        select = jnp.where(sel_mask, nt(sel_pick, facts), 0.0).astype(BF16)
        own = rows[y, first : first + ZC, :, :DY].astype(F32).reshape(TC, DY).astype(BF16)
        xe[g, seat] = nn(select, own).astype(BF16)
        for i, j in plane:
            px, py = plane_peer(i, j)
            send(xe.at[g, seat], xe.at[g, seat], 10 + g, (z, px, c, py))

    def expert(g):
        arrived(xe.at[g, pl.ds(0, X * Y - 1)], 10 + g)
        received = jnp.concatenate(
            [
                xe[g, j * X : (j + 1) * X].reshape(X * SC, DY)
                for j in range(Y)
            ],
            axis=1,
        )
        gate_pre = nt(received, we[:, 0].reshape(F, D))
        up_pre = nt(received, we[:, 1].reshape(F, D))
        hidden = (gate_pre / (1.0 + jnp.exp(-gate_pre)) * up_pre).astype(BF16)
        partial = nn(hidden, we[:, 2].reshape(F, D))
        for i in range(X):
            for j in range(Y):
                pb[g, j * X + i] = partial[
                    i * SC : (i + 1) * SC, j * DY : (j + 1) * DY
                ].astype(BF16)
        for i, j in plane:
            px, py = plane_peer(i, j)
            send(pb.at[g, py * X + px], pr.at[g, seat], 2 + g, (z, px, c, py))
        pr[g, seat] = pb[g, seat]

    def stacked(a, b):
        return jnp.concatenate([dw[k, :, a:b] for k in range(XC)], axis=0)

    def dense_part(g):
        first = g * ZC
        arrived(rows.at[pl.ds(0, Y - 1), pl.ds(first, ZC), :, pl.ds(0, DY)], 12 + g)
        line = jnp.concatenate(
            [
                rows[j, first : first + ZC, :, :DY].astype(F32).reshape(TC, DY).astype(BF16)
                for j in range(Y)
            ],
            axis=1,
        )
        dense_gate = nt(line, stacked(0, D))
        dense_up = nt(line, stacked(D, 2 * D))
        dense_hidden = (dense_gate / (1.0 + jnp.exp(-dense_gate)) * dense_up).astype(BF16)
        facts = rows[y, first : first + ZC, :, DY:].astype(F32).reshape(TC, 128).astype(BF16)
        shares = jnp.where(share_mask, nt(facts, share_pick), 0.0).astype(BF16)
        mixes = jnp.sum(
            jnp.where(mix_lanes, facts.astype(F32), 0.0), axis=1, keepdims=True
        )
        mixing[g] = (shares, nn(dense_hidden, stacked(2 * D, 2 * D + DY)) * mixes)

    def home(g):
        first = g * ZC
        arrived(pr.at[g, pl.ds(0, X * Y - 1)], 2 + g)
        served = jnp.zeros((SC, DY), F32)
        for k in range(X * Y):
            served = served + pr[g, k].astype(F32)
        served_high = served.astype(BF16)
        served_low = (served - served_high.astype(F32)).astype(BF16)
        stack = jnp.concatenate([served_high, served_low, served_high], axis=0)
        shares, dense = mixing[g]
        mixed = dense + nn(shares, stack)
        fb[first : first + ZC] = mixed.reshape(ZC, T, DY).astype(BF16)
        for to in range(first, first + ZC):

            @pl.when(z != to)
            def _(to=to):
                send(fb.at[to], fr.at[z], 6, (to, x, c, y))

            @pl.when(z == to)
            def _(to=to):
                fr[to] = fb[to]

    def spread_tokens(g):
        for j in range(1, Y):
            block = rows.at[y, pl.ds(g * ZC, ZC), :, pl.ds(0, DY)]
            send(block, block, 12 + g, (z, x, c, lax.rem(y + j, Y)))

    early = z < Z // 2
    gather(0)

    @pl.when(jnp.logical_not(early))
    def _():
        gather(1)

    spread_tokens(0)
    arrived(we.at[0], 1)
    expert(0)

    @pl.when(early)
    def _():
        gather(1)
        spread_tokens(1)

    @pl.when(jnp.logical_not(early))
    def _():
        expert(1)
        spread_tokens(1)

    arrived(dw.at[pl.ds(0, X)], 5)
    dense_part(0)
    home(0)

    @pl.when(early)
    def _():
        expert(1)

    dense_part(1)
    home(1)

    arrived(fr.at[pl.ds(0, Z - 1)], 6)
    combined = RESIDUAL_SCALE * settled_cols[y].astype(F32)
    combined = combined + jnp.sum(fr[...].astype(F32), axis=0)
    centre = jnp.sum(combined, axis=1, keepdims=True) / DY
    centred = combined - centre
    scatter = jnp.sum(centred * centred, axis=1, keepdims=True)
    stats[y] = jnp.where(lanes == 0, centre, jnp.where(lanes == 1, scatter, 0.0))
    for j in range(1, Y):
        send(stats.at[y], stats.at[y], 7, (z, x, c, lax.rem(y + j, Y)))
    ffn_gain = jnp.concatenate(
        [ffn_gain_ref[k : k + 1, :] for k in range(DY // 128)], axis=1
    )
    arrived(stats.at[pl.ds(0, Y - 1)], 7)
    every = [stats[j] for j in range(Y)]
    mean = sum(e[:, 0:1] for e in every) / Y
    var = sum(e[:, 1:2] + DY * (e[:, 0:1] - mean) * (e[:, 0:1] - mean) for e in every) / D
    out_ref[...] = ((combined - mean) * lax.rsqrt(var + 1e-05) * ffn_gain).astype(BF16)

    left_here(att.at[pl.ds(0, Y - 1)], 0)
    left_here(we.at[0], 1)
    left_here(dw.at[pl.ds(0, X - 1)], 4)
    left_here(dw.at[pl.ds(0, X)], 5)
    left_here(rows.at[y, pl.ds(0, Z - 1)], 8 + z // ZC)
    for g in range(CHUNKS):
        left_here(xe.at[g, pl.ds(0, X * Y - 1)], 10 + g)
        left_here(rows.at[pl.ds(0, Y - 1), pl.ds(g * ZC, ZC), :, pl.ds(0, DY)], 12 + g)
        left_here(pb.at[g, pl.ds(0, X * Y - 1)], 2 + g)
    left_here(fb.at[pl.ds(0, Z - 1)], 6)
    left_here(stats.at[pl.ds(0, Y - 1)], 7)


def hand_over(result_in, kv_in, result_out, kv_out, sem):
    copies = [
        pltpu.make_async_copy(result_in, result_out, sem.at[0]),
        pltpu.make_async_copy(kv_in, kv_out, sem.at[1]),
    ]
    for copy in copies:
        copy.start()
    for copy in copies:
        copy.wait()


def body(
    dims,
    tokens,
    kv_cache,
    lengths,
    w_query,
    w_key,
    w_value,
    break_bias,
    head_gain,
    w_output,
    attn_norm_gain,
    w_router,
    routes,
    expert_gate,
    expert_up,
    expert_down,
    dense_gate,
    dense_up,
    dense_down,
    mix_gate,
    ffn_norm_gain,
):
    Z, X, C, Y = dims
    T, D = tokens.shape
    DY = D // Y
    L, HD2 = kv_cache.shape[2:]
    F = expert_gate.shape[1]
    FD = dense_gate.shape[1]
    FDP = -(-FD // 8) * 8
    ZS = Z * CAP
    experts = w_router.shape[1]
    anywhere = pl.BlockSpec(memory_space=pl.ANY)
    V = pltpu.VMEM
    result, new_kv = pl.pallas_call(
        functools.partial(layer_kernel, dims),
        out_shape=(V((T, DY), BF16), V((T, HD2), BF16)),
        in_specs=[anywhere] * 20,
        out_specs=(pl.BlockSpec(memory_space=pltpu.VMEM),) * 2,
        scratch_shapes=[
            V((T, D), BF16),
            V((T, L, HD2), BF16),
            V((D, HD2), BF16),
            V((2, HD2 // 2, D), BF16),
            V((HD2, D), BF16),
            V((experts, D), BF16),
            V((C, 3, F, D), BF16),
            V((FD, D), BF16),
            V((FD, D), BF16),
            V((FD, DY), BF16),
            V((X * C, FDP, 2 * D + DY), BF16),
            V((Y, T, D), BF16),
            V((Y, T, DY), BF16),
            V((Y, Z, T, DY + 128), BF16),
            V((CHUNKS, X * Y, ZS // CHUNKS, DY), BF16),
            V((CHUNKS, X * Y, ZS // CHUNKS, DY), BF16),
            V((CHUNKS, X * Y, ZS // CHUNKS, DY), BF16),
            V((Z, T, DY), BF16),
            V((Z, T, DY), BF16),
            V((Y, T, 128), F32),
            pltpu.SMEM((T,), jnp.int32),
            pltpu.SMEM((2,), F32),
            pltpu.SMEM((2, T), jnp.int32),
            V((1, HD2), F32),
            V((D // 128, 128), F32),
            V((D // 128, 128), BF16),
            V((DY // 128, 128), F32),
            pltpu.SemaphoreType.DMA((17,)),
            pltpu.SemaphoreType.DMA((14,)),
            pltpu.SemaphoreType.DMA((14,)),
            pltpu.SemaphoreType.REGULAR((dims[0],)),
            pltpu.SemaphoreType.REGULAR,
            pltpu.SemaphoreType.REGULAR,
            pltpu.SemaphoreType.REGULAR,
            pltpu.SemaphoreType.REGULAR,
        ],
        compiler_params=pltpu.CompilerParams(
            collective_id=0, has_side_effects=True, vmem_limit_bytes=64000000
        ),
        name="layer",
    )(
        tokens,
        kv_cache.reshape(T, L, HD2),
        lengths,
        w_query,
        w_key.T,
        w_value.T,
        break_bias,
        head_gain.reshape(1, HD2),
        w_output,
        attn_norm_gain.reshape(D // 128, 128),
        w_router.T,
        routes.T,
        expert_gate.T,
        expert_up.T,
        expert_down,
        dense_gate.T,
        dense_up.T,
        dense_down,
        mix_gate.reshape(D // 128, 128),
        ffn_norm_gain.reshape(DY // 128, 128),
    )
    result, new_kv = pl.pallas_call(
        hand_over,
        out_shape=(
            jax.ShapeDtypeStruct((T, DY), BF16),
            jax.ShapeDtypeStruct((T, HD2), BF16),
        ),
        in_specs=[pl.BlockSpec(memory_space=pltpu.VMEM)] * 2,
        out_specs=(anywhere, anywhere),
        scratch_shapes=[pltpu.SemaphoreType.DMA((2,))],
        compiler_params=pltpu.CompilerParams(vmem_limit_bytes=1024 * 1024),
        name="hand_over",
    )(result, new_kv)
    return result, new_kv.reshape(T, 1, HD2)


def solution(mesh):
    cores = 2
    ep, tp = mesh.shape["ep"], mesh.shape["tp"]
    dims = (ep // (4 * cores), 4, cores, tp)
    split = Mesh(mesh.devices.reshape(dims), EP_TP)
    return jax.shard_map(
        functools.partial(body, dims),
        mesh=split,
        in_specs=(
            P(EP, None),
            P(EP, "tp", None, None),
            P(EP),
            P(None, "tp"),
            P(None, "tp"),
            P(None, "tp"),
            P("tp"),
            P("tp"),
            P("tp", None),
            P(),
            P(),
            P(EP, None),
            P(None, EP_TP),
            P(None, EP_TP),
            P(EP_TP, None),
            P(None, EP),
            P(None, EP),
            P(EP, "tp"),
            P(),
            P("tp"),
        ),
        out_specs=(P(EP, "tp"), P(EP, "tp", None)),
        check_vma=False,
    )
```
